512 devices in a mesh: sp: 128 (over z, x, core), tp: 4 (over y).
Axes of the slice: x: 4, y: 4, z: 16, core: 2. Of those that a mesh axis runs over, the one named last changes fastest.
Arguments:
- queries: bfloat16 [32768, 1024], P('sp', 'tp'), may hold values from -6 to 6
- keys: bfloat16 [32768, 1024], P('sp', 'tp'), may hold values from -6 to 6
- values: bfloat16 [32768, 2048], P('sp', 'tp'), may hold values from -6 to 6
- gate_code: bfloat16 [32768, 32], P('sp'), may hold values from -5.5 to 5.5
- gate_up: bfloat16 [32, 1024], P(None, 'tp'), may hold values from -1 to 1
- gate_bias: float32 [1024], P('tp'), as said below
- gla_gain: float32 [256], replicated, may hold values from 0.1 to 1.9
- conv_input: bfloat16 [32768, 2048], P('sp', 'tp'), may hold values from -6 to 6
- conv_gate: bfloat16 [32768, 2048], P('sp', 'tp'), may hold values from -6 to 6
- conv_taps: float32 [3, 2048], P(None, 'tp'), may hold values from -3.5 to 3.5
- out_gla: bfloat16 [2048, 2048], P('tp', 'sp'), may hold values from -0.09375 to 0.09375
- out_conv: bfloat16 [2048, 2048], P('tp', 'sp'), may hold values from -0.09375 to 0.09375
Outputs:
- mixed: bfloat16 [32768, 2048], P(('sp', 'tp'))
The draws below stay inside these ranges and needn't reach their ends.
Inputs may be any that keep to these rules, and one draw needn't show every extreme that they name: `gate_bias`: every bias is at least 1.5, so every decay per step lies strictly between 0 and 1.
All inputs are finite; a program needn't handle non-finite values.
Results may differ from the reference program's by a relative error of at most 0.028.
Values may be sent and summed in bfloat16 or wider, within the bound.
A program may use at most 64 MiB of HBM per device.

```python
import math
import jax
import jax.numpy as jnp
from jax import lax

D = 2048
HEAD_TOTAL = 8
KEY_WIDTH = 128
HEAD_V = 256
RANK = 32
CONV = 2048
TAPS = 3
SEGMENT_LENGTH = 64
TOK_DEV = 256
TOKENS = 32768
KEYS = 1024
VALS = 2048
N_SP = 128
N_TP = 4


def draw_gate_code(key, part):
    noise_key, shift_key = jax.random.split(jax.random.fold_in(key, 11))
    block_count = TOKENS // 128
    noise = jnp.clip(jax.random.normal(noise_key, (TOKENS, RANK), jnp.float32), -3.5, 3.5)
    shifts = jax.random.uniform(shift_key, (block_count, 1, RANK), jnp.float32, -1.5, 1.5)
    full = noise.reshape(block_count, 128, RANK) + shifts
    return full.reshape(TOKENS, RANK).astype(jnp.bfloat16)


def draw_gate_bias(key, part):
    pick_key, slow_key, fast_key = jax.random.split(jax.random.fold_in(key, 23), 3)
    base = math.log(TOKENS / 16.0) + 1.5
    slow_head = jax.random.permutation(pick_key, HEAD_TOTAL) < HEAD_TOTAL // 2
    slow_value = base + jax.random.uniform(slow_key, (HEAD_TOTAL, KEY_WIDTH), jnp.float32, -0.5, 0.5)
    fast_value = jax.random.uniform(fast_key, (HEAD_TOTAL, KEY_WIDTH), jnp.float32, 1.5, 2.5)
    chosen = jnp.where(slow_head[:, None], slow_value, fast_value)
    return chosen.reshape(HEAD_TOTAL * KEY_WIDTH).astype(jnp.float32)


def block_levels(own_key, extent, shards, smallest, high):
    level, own = 1.0, jax.random.fold_in(own_key, 6)
    for position, shards_of in shards:
        steps = jnp.exp(jax.random.uniform(jax.random.fold_in(own, position), (shards_of,), jnp.float32, smallest / len(shards), high / len(shards)))
        level = level * jnp.repeat(steps, extent[position] // shards_of).reshape([-1 if axis == position else 1 for axis in range(len(extent))])
    return level


def normal_values(own_key, extent, spread, limit, cuts=(), held_as=jnp.bfloat16):
    values = spread * jax.random.normal(own_key, extent, jnp.float32)
    if cuts:
        values = values * block_levels(own_key, extent, cuts, -0.22, 0.18)
    return jnp.clip(values, -limit, limit).astype(held_as)


def setup_inputs(seed: int = 0) -> dict:
    streams_of = jax.random.split(jax.random.key(seed), 13)
    return {
        "queries": normal_values(streams_of[0], (TOKENS, KEYS), 1.0, 6.0, ((0, 128), (1, 4))),
        "keys": normal_values(streams_of[1], (TOKENS, KEYS), 1.0, 6.0, ((0, 128), (1, 4))),
        "values": normal_values(streams_of[2], (TOKENS, VALS), 1.0, 6.0, ((0, 128), (1, 4))),
        "gate_code": draw_gate_code(jax.random.fold_in(streams_of[12], 71), 0),
        "gate_up": normal_values(streams_of[4], (RANK, KEYS), RANK ** -0.5, 1.0, ((1, 4),)),
        "gate_bias": draw_gate_bias(jax.random.fold_in(streams_of[12], 71), 0),
        "gla_gain": jnp.clip(1.0 + 0.18 * jax.random.normal(streams_of[6], (HEAD_V,), jnp.float32), 0.1, 1.9),
        "conv_input": normal_values(streams_of[7], (TOKENS, CONV), 1.0, 6.0, ((0, 128), (1, 4))),
        "conv_gate": normal_values(streams_of[8], (TOKENS, CONV), 1.0, 6.0, ((0, 128), (1, 4))),
        "conv_taps": normal_values(streams_of[9], (TAPS, CONV), TAPS ** -0.5, 3.5, ((1, 4),), jnp.float32),
        "out_gla": normal_values(streams_of[10], (VALS, D), (VALS + CONV) ** -0.5, 0.09375, ((0, 4), (1, 128))),
        "out_conv": normal_values(streams_of[11], (CONV, D), (VALS + CONV) ** -0.5, 0.09375, ((0, 4), (1, 128))),
    }


softness_divisor = 16.0
epsilon = 1.0

def reference(queries, keys, values, gate_code, gate_up, gate_bias, gla_gain, conv_input, conv_gate, conv_taps, out_gla, out_conv):
    segment_count = TOK_DEV // SEGMENT_LENGTH
    reach_rows = TAPS - 1
    val_group = HEAD_TOTAL * HEAD_V // N_TP
    conv_group = CONV // N_TP

    def per_block(carried, inputs):
        carried_state, last_rows = carried
        query_blk, key_blk, value_blk, code_blk, input_blk, gate_blk = inputs
        gate_score = jnp.dot(code_blk, gate_up, preferred_element_type=jnp.float32) + gate_bias
        decay_logarithm = (jax.nn.log_sigmoid(gate_score) / softness_divisor).reshape(segment_count, SEGMENT_LENGTH, HEAD_TOTAL, KEY_WIDTH)
        inside = jnp.cumsum(decay_logarithm, axis=1)
        seg_total = inside[:, -1]
        key_four = key_blk.reshape(segment_count, SEGMENT_LENGTH, HEAD_TOTAL, KEY_WIDTH).astype(jnp.float32)
        scaled_keys = (key_four * jnp.exp(seg_total[:, None] - inside)).astype(jnp.bfloat16)
        value_four = value_blk.reshape(segment_count, SEGMENT_LENGTH, HEAD_TOTAL, HEAD_V).astype(jnp.float32)
        update = jnp.einsum('nshk,nshv->nhkv', scaled_keys.astype(jnp.float32), value_four)

        def advance(running, segment_pair):
            running = jnp.exp(segment_pair[0])[..., None] * running + segment_pair[1]
            return (running, running)
        carried_state, states = lax.scan(advance, carried_state, (seg_total, update))
        low_states = lax.optimization_barrier(states.astype(jnp.bfloat16)).astype(jnp.float32)
        query_four = query_blk.reshape(segment_count, SEGMENT_LENGTH, HEAD_TOTAL, KEY_WIDTH).astype(jnp.float32)
        readout = jnp.einsum('nshk,nhkv->nshv', query_four, low_states)
        norm_scale = lax.rsqrt(lax.optimization_barrier(jnp.mean(readout * readout, axis=-1, keepdims=True)) + epsilon)
        gla_mix = (readout * norm_scale * gla_gain).astype(jnp.bfloat16).reshape(TOK_DEV, HEAD_TOTAL * HEAD_V)
        extended = jnp.concatenate([last_rows, input_blk], axis=0)
        convolved = jnp.zeros((TOK_DEV, CONV), jnp.float32)
        for offset in range(TAPS):
            convolved = convolved + conv_taps[offset] * extended[offset:offset + TOK_DEV].astype(jnp.float32)
        conv_mix = (gate_blk.astype(jnp.float32) * convolved).astype(jnp.bfloat16)
        summed = jnp.zeros((TOK_DEV, D), jnp.float32)
        for group_index in range(N_TP):
            val_lo = group_index * val_group
            conv_lo = group_index * conv_group
            part_sum = jnp.dot(gla_mix[:, val_lo:val_lo + val_group], out_gla[val_lo:val_lo + val_group], preferred_element_type=jnp.float32)
            part_sum = part_sum + jnp.dot(conv_mix[:, conv_lo:conv_lo + conv_group], out_conv[conv_lo:conv_lo + conv_group], preferred_element_type=jnp.float32)
            summed = summed + lax.optimization_barrier(part_sum.astype(jnp.bfloat16)).astype(jnp.float32)
        return ((carried_state, input_blk[TOK_DEV - reach_rows:]), summed.astype(jnp.bfloat16))

    def blocks(source):
        return source.reshape(N_SP, TOK_DEV, source.shape[-1])
    initial = (jnp.zeros((HEAD_TOTAL, KEY_WIDTH, HEAD_V), jnp.float32), jnp.zeros((reach_rows, CONV), jnp.bfloat16))
    sliced = (blocks(queries), blocks(keys), blocks(values), blocks(gate_code), blocks(conv_input), blocks(conv_gate))
    _, outputs = lax.scan(per_block, initial, sliced)
    return outputs.reshape(TOKENS, D)
```

```python
import functools

import jax
import jax.numpy as jnp
from jax import lax
from jax.experimental import pallas as pl
from jax.experimental.pallas import tpu as pltpu
from jax.sharding import PartitionSpec as P

MESH = pl.DeviceIdType.MESH
F32, BF16 = jnp.float32, jnp.bfloat16

NX, NC = 4, 2
KW, HV, SEG = 128, 256, 64
HEADS = 2
ROWS = 256
SEGS = ROWS // SEG
NCHUNK = 8
CW = 256
ORDER = (0, 1, -1, 2, -2, 3, -3, 4)
X_ORDER = (1, 3, 2)
NEAR = (1, 2, 3, 5, 6)
A_SEND = (1, 2, -1, -2, -3)
B_SEND = (5, 10)
NT = (((1,), (1,)), ((), ()))
TN = (((0,), (0,)), ((), ()))


def terms(a):
    high = a.astype(BF16).astype(F32)
    rest = a - high
    mid = rest.astype(BF16).astype(F32)
    return [high, mid, rest - mid]


def decay_rows(*decays):
    rows = [r for a in decays for r in terms(a)]
    rows.append(jnp.zeros((16 - len(rows), KW), F32))
    return jnp.concatenate(rows, axis=0).astype(BF16)


def decay_of(block, which=0):
    b = block.astype(F32)
    i = 3 * which
    return b[i : i + 1] + b[i + 1 : i + 2] + b[i + 2 : i + 3]


def chain(earlier, latter):
    return earlier[0] * latter[0], latter[0] * earlier[1] + latter[1]


def only_if(valid, pair):
    return jnp.where(valid, pair[0], 1.0), jnp.where(valid, pair[1], 0.0)


def layer_kernel(
    nz,
    nt,
    q, k, v, code, up, bias, gain, cin, cgate, taps, wblk,
    out,
    wt, states, through, ubuf, u0, pbuf, prec, abuf, arec, wbuf, brec, rbuf, sin,
    ctail, ext, mix, part, rel, comb, from_left, from_right,
    zsem, fsem, xs_sem, rs_sem, ls_sem, fs_sem, wd_sem,
    u0_sem, p_sem, a_sem, b_sem, r_sem, sin_sem, c_sem,
    rel_sem, left_sem, right_sem, tail_send,
):
    s = lax.axis_index("sp")
    t = lax.axis_index("tp")
    ns = nz * NX * NC
    c = lax.rem(s, NC)
    x = lax.rem(s // NC, NX)
    z = s // (NC * NX)

    def chip(zz, xx, cc):
        return {"sp": (zz * NX + xx) * NC + cc, "tp": t}

    def along_z(d):
        return chip(lax.rem(z + d + nz, nz), x, c)

    def along_x(d):
        return chip(z, lax.rem(x + d + NX, NX), c)

    def along_y(d):
        return {"sp": s, "tp": lax.rem(t + d + nt, nt)}

    def next_in_order(d):
        return {"sp": lax.rem(s + d + ns, ns), "tp": t}

    partner = chip(z, x, 1 - c)

    def rdma(src, dst, send, recv, dev):
        return pltpu.make_async_remote_copy(
            src_ref=src, dst_ref=dst, send_sem=send, recv_sem=recv,
            device_id=dev, device_id_type=MESH,
        )

    barrier = pltpu.get_barrier_semaphore()

    def greet(dev):
        pl.semaphore_signal(barrier, inc=1, device_id=dev, device_id_type=MESH)

    greet(partner)
    for d in (1, 2, 3):
        greet(along_x(d))
    for d in (1, -1):
        greet(along_y(d))
        greet(next_in_order(d))

    @pl.when(c == 0)
    def _():
        greet(along_z(1))
        greet(along_z(-1))

    @pl.when(c == 1)
    def _():
        for d in NEAR:
            greet(along_z(d))
            greet(along_z(-d))

    score = jnp.dot(code[...], up[...], preferred_element_type=F32) + bias[...]
    log_decay = (jnp.minimum(score, 0.0) - jnp.log1p(jnp.exp(-jnp.abs(score)))) / 16.0
    row = lax.broadcasted_iota(jnp.int32, (SEG, SEG), 0)
    col = lax.broadcasted_iota(jnp.int32, (SEG, SEG), 1)
    later = (col > row).astype(F32)
    acc = [None] * HEADS
    thr = None
    for n in range(SEGS):
        here = log_decay[n * SEG : (n + 1) * SEG]
        rest = jnp.dot(
            later, here, preferred_element_type=F32, precision=lax.Precision.HIGHEST
        )
        scaled = (k[n * SEG : (n + 1) * SEG, :].astype(F32) * jnp.exp(rest)).astype(BF16)
        seg_decay = jnp.exp(rest[0:1] + here[0:1])
        thr = seg_decay if n == 0 else thr * seg_decay
        through[n] = jnp.broadcast_to(thr, (8, HEADS * KW))
        for h in range(HEADS):
            update = lax.dot_general(
                v[n * SEG : (n + 1) * SEG, h * HV : (h + 1) * HV],
                scaled[:, h * KW : (h + 1) * KW],
                TN,
                preferred_element_type=F32,
            )
            if n == 0:
                acc[h] = update
            else:
                acc[h] = acc[h] * seg_decay[:, h * KW : (h + 1) * KW] + update
            states[n, h * HV : (h + 1) * HV, :] = acc[h]
    for h in range(HEADS):
        ubuf[h * HV : (h + 1) * HV, :] = acc[h].astype(BF16)
    ubuf[HEADS * HV :, :] = decay_rows(thr[:, :KW], thr[:, KW:])

    @pl.when(c == 0)
    def _():
        wt[z, x, 0:16, :] = wblk[...]
        pl.semaphore_wait(barrier, 10)

    @pl.when(c == 1)
    def _():
        pl.semaphore_wait(barrier, 18)

    tail_copy = rdma(
        cin.at[ROWS - 16 : ROWS], ctail, c_sem.at[0], c_sem.at[1], next_in_order(1)
    )

    def conv():
        tail_copy.wait_recv()
        ext[8:, :] = cin[...].astype(F32)
        ext[0:8, :] = jnp.where(s == 0, 0.0, ctail[...].astype(F32)[8:16])
        done = taps[0:1] * ext[6 : 6 + ROWS, :]
        done = done + taps[1:2] * ext[7 : 7 + ROWS, :]
        done = done + taps[2:3] * ext[8 : 8 + ROWS, :]
        mix[:, HEADS * HV :] = (cgate[...].astype(F32) * done).astype(BF16)

    def read_out(incoming):
        for h in range(HEADS):
            for n in range(SEGS):
                decay = through[n, 0:1, h * KW : (h + 1) * KW]
                state = states[n, h * HV : (h + 1) * HV, :] + decay * incoming(h)
                got = lax.dot_general(
                    q[n * SEG : (n + 1) * SEG, h * KW : (h + 1) * KW],
                    state.astype(BF16),
                    NT,
                    preferred_element_type=F32,
                )
                scale = lax.rsqrt(jnp.mean(got * got, axis=-1, keepdims=True) + 1.0)
                mix[n * SEG : (n + 1) * SEG, h * HV : (h + 1) * HV] = (
                    got * scale * gain[...]
                ).astype(BF16)

    def block_copy(rr, xx, send, dev):
        return rdma(wt.at[rr, xx], wt.at[rr, xx], send, zsem.at[rr, xx], dev)

    def pass_on(rr):
        rdma(wt.at[rr], wt.at[rr], fs_sem, fsem.at[rr], partner).start()

    def row_at(d):
        return lax.rem(z + d + nz, nz)

    @pl.when(c == 0)
    def _():
        rdma(ubuf, u0, u0_sem.at[0], u0_sem.at[1], partner).start()
        tail_copy.start()
        rdma(wblk, wt.at[z, x, 16:32], wd_sem.at[0], wd_sem.at[1], partner).wait_recv()
        for d in X_ORDER:
            block_copy(z, x, xs_sem, along_x(d)).start()
        block_copy(z, x, rs_sem, along_z(1)).start()
        block_copy(z, x, ls_sem, along_z(-1)).start()
        conv()
        for d in X_ORDER:
            xx = lax.rem(x + d, NX)
            block_copy(z, xx, xs_sem, along_x(d)).wait_recv()
            block_copy(z, xx, rs_sem, along_z(1)).start()
            block_copy(z, xx, ls_sem, along_z(-1)).start()
        pass_on(z)

        @pl.loop(1, nz // 2 - 1)
        def _(step):
            up_row, down_row = row_at(-step), row_at(step)
            for d in (0,) + X_ORDER:
                xx = lax.rem(x + d, NX)
                block_copy(up_row, xx, rs_sem, along_z(1)).wait_recv()
                block_copy(up_row, xx, rs_sem, along_z(1)).start()
                block_copy(down_row, xx, ls_sem, along_z(-1)).wait_recv()
                block_copy(down_row, xx, ls_sem, along_z(-1)).start()
            pass_on(up_row)
            pass_on(down_row)

        up_row, down_row = row_at(1 - nz // 2), row_at(nz // 2 - 1)
        for d in (0,) + X_ORDER:
            xx = lax.rem(x + d, NX)
            block_copy(up_row, xx, rs_sem, along_z(1)).wait_recv()
            block_copy(up_row, xx, rs_sem, along_z(1)).start()
            block_copy(down_row, xx, ls_sem, along_z(-1)).wait_recv()
        pass_on(up_row)
        pass_on(down_row)
        far = row_at(nz // 2)
        for d in (0,) + X_ORDER:
            block_copy(far, lax.rem(x + d, NX), rs_sem, along_z(1)).wait_recv()
        pass_on(far)

        rdma(sin, sin, sin_sem.at[0], sin_sem.at[1], partner).wait_recv()
        read_out(
            lambda h: jnp.concatenate([sin[2 * h], sin[2 * h + 1]], axis=0).astype(F32)
        )

    @pl.when(c == 1)
    def _():
        rdma(wblk, wt.at[z, x, 16:32], wd_sem.at[0], wd_sem.at[1], partner).start()
        tail_copy.start()
        rdma(ubuf, u0, u0_sem.at[0], u0_sem.at[1], partner).wait_recv()
        first = [decay_of(u0[HEADS * HV :, :], h) for h in range(HEADS)]
        whole = [thr[:, h * KW : (h + 1) * KW] * first[h] for h in range(HEADS)]
        for i in range(NX):
            h, lo = i // 2, i * KW
            both = (
                u0[lo : lo + KW, :].astype(F32) * thr[:, h * KW : (h + 1) * KW]
                + acc[h][(i % 2) * KW : (i % 2 + 1) * KW]
            )
            pbuf[i, 0:KW, :] = both.astype(BF16)
            pbuf[i, KW:, :] = decay_rows(whole[h])
        for j, d in enumerate((1, 3, 2)):
            rdma(
                pbuf.at[lax.rem(x + d, NX)], prec.at[x],
                p_sem.at[0], p_sem.at[1 + d], along_x(d),
            ).start()
        prec[x] = pbuf[x]
        for d in (1, 2, 3):
            rdma(
                pbuf.at[0], prec.at[lax.rem(x - d + NX, NX)],
                p_sem.at[0], p_sem.at[1 + d], along_x(d),
            ).wait_recv()

        def pair_in(ref, i):
            return decay_of(ref[i, KW:, :]), ref[i, 0:KW, :].astype(F32)

        chips = [pair_in(prec, i) for i in range(NX)]
        plane = chips[0]
        for i in range(1, NX):
            plane = chain(plane, chips[i])
        abuf[0:KW, :] = plane[1].astype(BF16)
        abuf[KW:, :] = decay_rows(plane[0])
        for j, d in enumerate(A_SEND):
            rdma(abuf, arec.at[j], a_sem.at[5], a_sem.at[j], along_z(d)).start()
        conv()
        for j, d in enumerate(A_SEND):
            rdma(abuf, arec.at[j], a_sem.at[5], a_sem.at[j], along_z(d)).wait_recv()
        back1, back2, ahead1, ahead2, ahead3 = (pair_in(arec, j) for j in range(5))
        inner = z <= nz - 4
        window = only_if(inner & (z >= 2), back2)
        window = chain(window, only_if(inner & (z >= 1), back1))
        window = chain(window, only_if(inner, plane))
        window = chain(window, only_if(inner | (z == nz - 1), ahead1))
        window = chain(window, only_if(inner | (z >= nz - 2), ahead2))
        wbuf[0:KW, :] = window[1].astype(BF16)
        wbuf[KW:, :] = decay_rows(window[0])
        for j, d in enumerate(B_SEND):
            rdma(wbuf, brec.at[j], b_sem.at[2], b_sem.at[j], along_z(d)).start()
        oldest = only_if(z >= nz - 1, ahead1)
        oldest = chain(oldest, only_if(z >= nz - 2, ahead2))
        oldest = chain(oldest, only_if(z >= nz - 3, ahead3))
        newest = chain(only_if(z >= 2, back2), only_if(z >= 1, back1))
        for j, d in enumerate(B_SEND):
            rdma(wbuf, brec.at[j], b_sem.at[2], b_sem.at[j], along_z(d)).wait_recv()
        before = chain(oldest, only_if(z >= 8, pair_in(brec, 1)))
        before = chain(before, only_if(z >= 3, pair_in(brec, 0)))
        before = chain(before, newest)
        run = before[1]
        for i in range(NX):
            rbuf[i] = run.astype(BF16)
            if i < NX - 1:
                run = chips[i][0] * run + chips[i][1]
        for d in (1, 3, 2):
            rdma(
                rbuf.at[lax.rem(x + d, NX)], sin.at[x],
                r_sem.at[0], r_sem.at[1 + d], along_x(d),
            ).start()
        sin[x] = rbuf[x]
        for d in (1, 2, 3):
            rdma(
                rbuf.at[0], sin.at[lax.rem(x - d + NX, NX)],
                r_sem.at[0], r_sem.at[1 + d], along_x(d),
            ).wait_recv()
        rdma(sin, sin, sin_sem.at[0], sin_sem.at[1], partner).start()

        def incoming(h):
            got = jnp.concatenate([sin[2 * h], sin[2 * h + 1]], axis=0).astype(F32)
            return first[h] * got + u0[h * HV : (h + 1) * HV, :].astype(F32)

        read_out(incoming)

    right, left = along_y(1), along_y(-1)
    opposite, at_right, at_left = (lax.rem(t + d, nt) for d in (2, 1, 3))
    zc = z // 2
    columns = [lax.rem(zc + d + NCHUNK, NCHUNK) for d in ORDER]
    for o, j in enumerate(columns):
        @pl.when(c == 1)
        def _():
            for i in range(2):
                rdma(
                    wt.at[2 * j + i], wt.at[2 * j + i], fs_sem, fsem.at[2 * j + i], partner
                ).wait_recv()

        w = wt[pl.ds(2 * j, 2)].reshape(CW, 2 * HEADS * HV)
        got = lax.dot_general(mix[...], w, NT, preferred_element_type=F32)
        part[o] = got.astype(BF16).reshape(nt, ROWS // nt, CW)
        rdma(
            part.at[o, opposite], rel.at[o], tail_send.at[0], rel_sem.at[o],
            right if o % 2 == 0 else left,
        ).start()
    for o in range(NCHUNK):
        if o % 2 == 0:
            rdma(
                part.at[o, at_left], from_right.at[o], tail_send.at[1],
                right_sem.at[o], left,
            ).start()
        else:
            rdma(
                part.at[o, at_right], from_left.at[o], tail_send.at[1],
                left_sem.at[o], right,
            ).start()
    for o in range(NCHUNK):
        to = right if o % 2 == 0 else left
        rdma(part.at[o, 0], rel.at[o], tail_send.at[0], rel_sem.at[o], to).wait_recv()
        mine = part[o, at_right if o % 2 == 0 else at_left]
        comb[o] = (rel[o].astype(F32) + mine.astype(F32)).astype(BF16)
        if o % 2 == 0:
            rdma(comb.at[o], from_left.at[o], tail_send.at[2], left_sem.at[o], right).start()
        else:
            rdma(comb.at[o], from_right.at[o], tail_send.at[2], right_sem.at[o], left).start()
    for o, j in enumerate(columns):
        rdma(comb.at[o], from_left.at[o], tail_send.at[2], left_sem.at[o], right).wait_recv()
        rdma(comb.at[o], from_right.at[o], tail_send.at[2], right_sem.at[o], left).wait_recv()
        total = part[o, t].astype(F32) + from_left[o].astype(F32) + from_right[o].astype(F32)
        out[:, pl.ds(pl.multiple_of(j * CW, CW), CW)] = total.astype(BF16)

    for i in range(3):
        rdma(comb, rel, tail_send.at[i], rel_sem.at[0], right).wait_send()
    tail_copy.wait_send()

    @pl.when(c == 0)
    def _():
        rdma(ubuf, u0, u0_sem.at[0], u0_sem.at[1], partner).wait_send()
        rdma(wt.at[0, 0:3], wt.at[0, 0:3], xs_sem, zsem.at[0, 0], partner).wait_send()
        half = nz // 2
        rdma(wt.at[0:half], wt.at[0:half], rs_sem, zsem.at[0, 0], partner).wait_send()
        rdma(
            wt.at[0 : half - 1], wt.at[0 : half - 1], ls_sem, zsem.at[0, 0], partner
        ).wait_send()
        rdma(wt, wt, fs_sem, fsem.at[0], partner).wait_send()

    @pl.when(c == 1)
    def _():
        rdma(wblk, wt.at[0, 0, 0:16], wd_sem.at[0], wd_sem.at[1], partner).wait_send()
        rdma(pbuf.at[0:3], prec.at[0:3], p_sem.at[0], p_sem.at[1], partner).wait_send()
        rdma(arec, arec, a_sem.at[5], a_sem.at[0], partner).wait_send()
        rdma(brec, brec, b_sem.at[2], b_sem.at[0], partner).wait_send()
        rdma(rbuf.at[0:3], sin.at[0:3], r_sem.at[0], r_sem.at[1], partner).wait_send()
        rdma(sin, sin, sin_sem.at[0], sin_sem.at[1], partner).wait_send()


def solution(mesh):
    nt = mesh.shape["tp"]
    nz = mesh.shape["sp"] // (NX * NC)

    def step(
        queries, keys, values, gate_code, gate_up, gate_bias, gla_gain,
        conv_input, conv_gate, conv_taps, out_gla, out_conv,
    ):
        weights = jnp.concatenate([out_gla.T, out_conv.T], axis=1)
        width = HEADS * HV
        vm, dma = pltpu.VMEM, pltpu.SemaphoreType.DMA
        quarter = ROWS // nt
        scratch = [
            vm((nz, NX, 32, 2 * width), BF16),
            vm((SEGS, width, KW), F32),
            vm((SEGS, 8, HEADS * KW), F32),
            vm((width + 16, KW), BF16),
            vm((width + 16, KW), BF16),
            vm((NX, KW + 16, KW), BF16),
            vm((NX, KW + 16, KW), BF16),
            vm((KW + 16, KW), BF16),
            vm((5, KW + 16, KW), BF16),
            vm((KW + 16, KW), BF16),
            vm((2, KW + 16, KW), BF16),
            vm((NX, KW, KW), BF16),
            vm((NX, KW, KW), BF16),
            vm((16, width), BF16),
            vm((8 + ROWS, width), F32),
            vm((ROWS, 2 * width), BF16),
            vm((NCHUNK, nt, quarter, CW), BF16),
            vm((NCHUNK, quarter, CW), BF16),
            vm((NCHUNK, quarter, CW), BF16),
            vm((NCHUNK, quarter, CW), BF16),
            vm((NCHUNK, quarter, CW), BF16),
            dma((nz, NX)), dma((nz,)), dma, dma, dma, dma, dma((2,)),
            dma((2,)), dma((5,)), dma((6,)), dma((3,)), dma((5,)), dma((2,)), dma((2,)),
            dma((NCHUNK,)), dma((NCHUNK,)), dma((NCHUNK,)), dma((3,)),
        ]
        return pl.pallas_call(
            functools.partial(layer_kernel, nz, nt),
            out_shape=jax.ShapeDtypeStruct((quarter, 2048), BF16),
            in_specs=[pl.BlockSpec(memory_space=pltpu.VMEM)] * 11,
            out_specs=pl.BlockSpec(memory_space=pltpu.VMEM),
            scratch_shapes=scratch,
            compiler_params=pltpu.CompilerParams(collective_id=0, has_side_effects=True),
            name="layer",
        )(
            queries, keys, values, gate_code, gate_up, gate_bias[None], gla_gain[None],
            conv_input, conv_gate, conv_taps, weights,
        )

    return jax.shard_map(
        step,
        mesh=mesh,
        in_specs=(
            P("sp", "tp"), P("sp", "tp"), P("sp", "tp"), P("sp", None), P(None, "tp"),
            P("tp"), P(), P("sp", "tp"), P("sp", "tp"), P(None, "tp"),
            P("tp", "sp"), P("tp", "sp"),
        ),
        out_specs=P(("sp", "tp"), None),
        check_vma=False,
    )
```

```python
import functools

import jax
import jax.numpy as jnp
from jax import lax
from jax.experimental import pallas as pl
from jax.experimental.pallas import tpu as pltpu
from jax.sharding import PartitionSpec as P

MESH = pl.DeviceIdType.MESH
F32, BF16 = jnp.float32, jnp.bfloat16

NX, NC = 4, 2
KW, HV, SEG = 128, 256, 64
HEADS = 2
ROWS = 256
SEGS = ROWS // SEG
NCHUNK = 8
CW = 256
W, S = 1, 0
ORDER = (0, 1, -1, 2, -2, 3, -3, 4)
X_ORDER = (1, 3, 2)
NEAR = (1, 2, 3, 5, 6)
A_SEND = (1, 2, -1, -2, -3)
B_SEND = (5, 10)
Z_SENDS = {
    0: (1, -1, 5, -5), 5: (1, -1), -5: (1, -1), -1: (1,), 1: (-1,),
    4: (1,), 6: (-1,), 7: (-1,), -6: (1,), -4: (-1,),
}
ARRIVE_ORDER = (1, -1, 5, -5, 2, -2, 4, 6, -4, -6, 3, 7, -3, -7, 8)
LAG_R, LAG_F = 4, 7
NT = (((1,), (1,)), ((), ()))
TN = (((0,), (0,)), ((), ()))


def terms(a):
    high = a.astype(BF16).astype(F32)
    rest = a - high
    mid = rest.astype(BF16).astype(F32)
    return [high, mid, rest - mid]


def decay_rows(*decays):
    rows = [r for a in decays for r in terms(a)]
    rows.append(jnp.zeros((16 - len(rows), KW), F32))
    return jnp.concatenate(rows, axis=0).astype(BF16)


def decay_of(block, which=0):
    b = block.astype(F32)
    i = 3 * which
    return b[i : i + 1] + b[i + 1 : i + 2] + b[i + 2 : i + 3]


def chain(earlier, latter):
    return earlier[0] * latter[0], latter[0] * earlier[1] + latter[1]


def only_if(valid, pair):
    return jnp.where(valid, pair[0], 1.0), jnp.where(valid, pair[1], 0.0)


def layer_kernel(
    nz,
    nt,
    q, k, v, code, up, bias, gain, cin, cgate, taps, wgla, wconv,
    out,
    wt, states, through, ubuf, u0, pbuf, prec, abuf, arec, wbuf, brec, rbuf, sin,
    ctail, ext, mix, wblk, sout, part, rel, comb, from_left, from_right,
    zsem, fsem, ws_sem, fs_sem, wd_sem,
    u0_sem, p_sem, a_sem, b_sem, r_sem, sin_sem, c_sem,
    rel_sem, left_sem, right_sem, tail_send,
):
    s = lax.axis_index("sp")
    t = lax.axis_index("tp")
    ns = nz * NX * NC
    c = lax.rem(s, NC)
    x = lax.rem(s // NC, NX)
    z = s // (NC * NX)

    def chip(zz, xx, cc):
        return {"sp": (zz * NX + xx) * NC + cc, "tp": t}

    def along_z(d):
        return chip(lax.rem(z + d + nz, nz), x, c)

    def along_x(d):
        return chip(z, lax.rem(x + d + NX, NX), c)

    def along_y(d):
        return {"sp": s, "tp": lax.rem(t + d + nt, nt)}

    def next_in_order(d):
        return {"sp": lax.rem(s + d + ns, ns), "tp": t}

    partner = chip(z, x, 1 - c)

    def rdma(src, dst, send, recv, dev):
        return pltpu.make_async_remote_copy(
            src_ref=src, dst_ref=dst, send_sem=send, recv_sem=recv,
            device_id=dev, device_id_type=MESH,
        )

    barrier = pltpu.get_barrier_semaphore()

    def greet(dev):
        pl.semaphore_signal(barrier, inc=1, device_id=dev, device_id_type=MESH)

    greet(partner)
    for d in (1, 2, 3):
        greet(along_x(d))
    for d in (1, -1):
        greet(along_y(d))
        greet(next_in_order(d))

    @pl.when(c == W)
    def _():
        for d in (1, 5):
            greet(along_z(d))
            greet(along_z(-d))

    @pl.when(c == S)
    def _():
        for d in NEAR:
            greet(along_z(d))
            greet(along_z(-d))

    score = lax.dot_general(code[...], up[...], TN, preferred_element_type=F32) + bias[...]
    log_decay = (jnp.minimum(score, 0.0) - jnp.log1p(jnp.exp(-jnp.abs(score)))) / 16.0
    row = lax.broadcasted_iota(jnp.int32, (SEG, SEG), 0)
    col = lax.broadcasted_iota(jnp.int32, (SEG, SEG), 1)
    later = (col > row).astype(F32)
    acc = [None] * HEADS
    thr = None
    for n in range(SEGS):
        here = log_decay[n * SEG : (n + 1) * SEG]
        rest = jnp.dot(
            later, here, preferred_element_type=F32, precision=lax.Precision.HIGHEST
        )
        scaled = (k[n * SEG : (n + 1) * SEG, :].astype(F32) * jnp.exp(rest)).astype(BF16)
        seg_decay = jnp.exp(rest[0:1] + here[0:1])
        thr = seg_decay if n == 0 else thr * seg_decay
        through[n] = jnp.broadcast_to(thr, (8, HEADS * KW))
        for h in range(HEADS):
            update = lax.dot_general(
                v[n * SEG : (n + 1) * SEG, h * HV : (h + 1) * HV],
                scaled[:, h * KW : (h + 1) * KW],
                TN,
                preferred_element_type=F32,
            )
            if n == 0:
                acc[h] = update
            else:
                acc[h] = acc[h] * seg_decay[:, h * KW : (h + 1) * KW] + update
            states[n, h * HV : (h + 1) * HV, :] = acc[h]
    for h in range(HEADS):
        ubuf[h * HV : (h + 1) * HV, :] = acc[h].astype(BF16)
    ubuf[HEADS * HV :, :] = decay_rows(thr[:, :KW], thr[:, KW:])

    own_rows, other_rows = slice(16 * W, 16 * W + 16), slice(16 * S, 16 * S + 16)
    wblk[:, : HEADS * HV] = wgla[...]
    wblk[:, HEADS * HV :] = wconv[...]

    @pl.when(c == W)
    def _():
        wt[z, x, own_rows, :] = wblk[...]
        pl.semaphore_wait(barrier, 12)

    @pl.when(c == S)
    def _():
        pl.semaphore_wait(barrier, 18)

    tail_copy = rdma(
        cin.at[ROWS - 16 : ROWS], ctail, c_sem.at[0], c_sem.at[1], next_in_order(1)
    )

    def conv():
        tail_copy.wait_recv()
        ext[8:, :] = cin[...].astype(F32)
        ext[0:8, :] = jnp.where(s == 0, 0.0, ctail[...].astype(F32)[8:16])
        done = taps[0:1] * ext[6 : 6 + ROWS, :]
        done = done + taps[1:2] * ext[7 : 7 + ROWS, :]
        done = done + taps[2:3] * ext[8 : 8 + ROWS, :]
        mix[:, HEADS * HV :] = (cgate[...].astype(F32) * done).astype(BF16)

    def read_out(incoming):
        for h in range(HEADS):
            for n in range(SEGS):
                decay = through[n, 0:1, h * KW : (h + 1) * KW]
                state = states[n, h * HV : (h + 1) * HV, :] + decay * incoming(h)
                got = lax.dot_general(
                    q[n * SEG : (n + 1) * SEG, h * KW : (h + 1) * KW],
                    state.astype(BF16),
                    NT,
                    preferred_element_type=F32,
                )
                scale = lax.rsqrt(jnp.mean(got * got, axis=-1, keepdims=True) + 1.0)
                mix[n * SEG : (n + 1) * SEG, h * HV : (h + 1) * HV] = (
                    got * scale * gain[...]
                ).astype(BF16)

    def arrived(h):
        return jnp.concatenate([sin[2 * h], sin[2 * h + 1]], axis=0).astype(F32)

    def send_block(rr, xx, sem, dev):
        block = wt.at[rr, xx]
        rdma(block, block, ws_sem.at[sem], zsem.at[rr, xx], dev).start()

    def wait_block(rr, xx):
        block = wt.at[rr, xx]
        rdma(block, block, ws_sem.at[0], zsem.at[rr, xx], partner).wait_recv()

    def row_at(d):
        return lax.rem(z + d + nz, nz)

    def x_at(d):
        return lax.rem(x + d, NX)

    def arrive(d):
        if d != 0:
            wait_block(row_at(d), x)
        for to in Z_SENDS.get(d, ()):
            send_block(row_at(d), x, 0, along_z(to))
        for to in (1, 3):
            send_block(row_at(d), x, 1, along_x(to))

    def relay(d):
        near = 3 if d <= 0 else 1
        wait_block(row_at(d), x_at(near))
        send_block(row_at(d), x_at(near), 2, along_x(4 - near))

    def finish(d):
        far = 1 if d <= 0 else 3
        wait_block(row_at(d), x_at(far))
        wait_block(row_at(d), x_at(2))
        rr = row_at(d)
        rdma(wt.at[rr], wt.at[rr], fs_sem, fsem.at[rr], partner).start()

    @pl.when(c == W)
    def _():
        rdma(ubuf, u0, u0_sem.at[0], u0_sem.at[1], partner).start()
        tail_copy.start()
        rdma(wblk, wt.at[z, x, other_rows], wd_sem.at[0], wd_sem.at[1], partner).wait_recv()
        arrive(0)
        conv()
        order = (0,) + ARRIVE_ORDER
        for i in range(1, nz + LAG_F):
            if i < nz:
                arrive(order[i])
            if 0 <= i - LAG_R < nz:
                relay(order[i - LAG_R])
            if 0 <= i - LAG_F < nz:
                finish(order[i - LAG_F])
        rdma(sin, sin, sin_sem.at[0], sin_sem.at[1], partner).wait_recv()
        read_out(arrived)

    @pl.when(c == S)
    def _():
        rdma(wblk, wt.at[z, x, other_rows], wd_sem.at[0], wd_sem.at[1], partner).start()
        tail_copy.start()
        rdma(ubuf, u0, u0_sem.at[0], u0_sem.at[1], partner).wait_recv()

        def theirs(h, lo, hi):
            return (
                decay_of(u0[HEADS * HV :, :], h),
                u0[h * HV + lo : h * HV + hi, :].astype(F32),
            )

        def ours(h, lo, hi):
            return thr[:, h * KW : (h + 1) * KW], acc[h][lo:hi]

        first, second = (theirs, ours) if S == 1 else (ours, theirs)
        for i in range(NX):
            part_of = (i // 2, (i % 2) * KW, (i % 2 + 1) * KW)
            both = chain(first(*part_of), second(*part_of))
            pbuf[i, 0:KW, :] = both[1].astype(BF16)
            pbuf[i, KW:, :] = decay_rows(both[0])
        for j, d in enumerate((1, 3, 2)):
            rdma(
                pbuf.at[lax.rem(x + d, NX)], prec.at[x],
                p_sem.at[0], p_sem.at[1 + d], along_x(d),
            ).start()
        prec[x] = pbuf[x]
        for d in (1, 2, 3):
            rdma(
                pbuf.at[0], prec.at[lax.rem(x - d + NX, NX)],
                p_sem.at[0], p_sem.at[1 + d], along_x(d),
            ).wait_recv()

        def pair_in(ref, i):
            return decay_of(ref[i, KW:, :]), ref[i, 0:KW, :].astype(F32)

        chips = [pair_in(prec, i) for i in range(NX)]
        plane = chips[0]
        for i in range(1, NX):
            plane = chain(plane, chips[i])
        abuf[0:KW, :] = plane[1].astype(BF16)
        abuf[KW:, :] = decay_rows(plane[0])
        for j, d in enumerate(A_SEND):
            rdma(abuf, arec.at[j], a_sem.at[5], a_sem.at[j], along_z(d)).start()
        conv()
        for j, d in enumerate(A_SEND):
            rdma(abuf, arec.at[j], a_sem.at[5], a_sem.at[j], along_z(d)).wait_recv()
        back1, back2, ahead1, ahead2, ahead3 = (pair_in(arec, j) for j in range(5))
        inner = z <= nz - 4
        window = only_if(inner & (z >= 2), back2)
        window = chain(window, only_if(inner & (z >= 1), back1))
        window = chain(window, only_if(inner, plane))
        window = chain(window, only_if(inner | (z == nz - 1), ahead1))
        window = chain(window, only_if(inner | (z >= nz - 2), ahead2))
        wbuf[0:KW, :] = window[1].astype(BF16)
        wbuf[KW:, :] = decay_rows(window[0])
        for j, d in enumerate(B_SEND):
            rdma(wbuf, brec.at[j], b_sem.at[2], b_sem.at[j], along_z(d)).start()
        oldest = only_if(z >= nz - 1, ahead1)
        oldest = chain(oldest, only_if(z >= nz - 2, ahead2))
        oldest = chain(oldest, only_if(z >= nz - 3, ahead3))
        newest = chain(only_if(z >= 2, back2), only_if(z >= 1, back1))
        for j, d in enumerate(B_SEND):
            rdma(wbuf, brec.at[j], b_sem.at[2], b_sem.at[j], along_z(d)).wait_recv()
        before = chain(oldest, only_if(z >= 8, pair_in(brec, 1)))
        before = chain(before, only_if(z >= 3, pair_in(brec, 0)))
        before = chain(before, newest)
        run = before[1]
        for i in range(NX):
            rbuf[i] = run.astype(BF16)
            if i < NX - 1:
                run = chips[i][0] * run + chips[i][1]
        for d in (1, 3, 2):
            rdma(
                rbuf.at[lax.rem(x + d, NX)], sin.at[x],
                r_sem.at[0], r_sem.at[1 + d], along_x(d),
            ).start()
        sin[x] = rbuf[x]
        for d in (1, 2, 3):
            rdma(
                rbuf.at[0], sin.at[lax.rem(x - d + NX, NX)],
                r_sem.at[0], r_sem.at[1 + d], along_x(d),
            ).wait_recv()

        def after_first(h):
            decay, update = first(h, 0, HV)
            return decay * arrived(h) + update

        if S == 1:
            rdma(sin, sin, sin_sem.at[0], sin_sem.at[1], partner).start()
        else:
            for h in range(HEADS):
                sout[2 * h : 2 * h + 2] = after_first(h).astype(BF16).reshape(2, KW, KW)
            rdma(sout, sin, sin_sem.at[0], sin_sem.at[1], partner).start()
        read_out(after_first if S == 1 else arrived)

    right, left = along_y(1), along_y(-1)
    opposite, at_right, at_left = (lax.rem(t + d, nt) for d in (2, 1, 3))
    zc = z // 2
    columns = [lax.rem(zc + d + NCHUNK, NCHUNK) for d in ORDER]
    for o, j in enumerate(columns):
        @pl.when(c == S)
        def _():
            for i in range(2):
                rdma(
                    wt.at[2 * j + i], wt.at[2 * j + i], fs_sem, fsem.at[2 * j + i], partner
                ).wait_recv()

        w = wt[pl.ds(2 * j, 2)].reshape(CW, 2 * HEADS * HV)
        got = lax.dot_general(mix[...], w, NT, preferred_element_type=F32)
        part[o] = got.astype(BF16).reshape(nt, ROWS // nt, CW)
        rdma(
            part.at[o, opposite], rel.at[o], tail_send.at[0], rel_sem.at[o],
            right if o % 2 == 0 else left,
        ).start()
    for o in range(NCHUNK):
        if o % 2 == 0:
            rdma(
                part.at[o, at_left], from_right.at[o], tail_send.at[1],
                right_sem.at[o], left,
            ).start()
        else:
            rdma(
                part.at[o, at_right], from_left.at[o], tail_send.at[1],
                left_sem.at[o], right,
            ).start()
    for o in range(NCHUNK):
        to = right if o % 2 == 0 else left
        rdma(part.at[o, 0], rel.at[o], tail_send.at[0], rel_sem.at[o], to).wait_recv()
        mine = part[o, at_right if o % 2 == 0 else at_left]
        comb[o] = (rel[o].astype(F32) + mine.astype(F32)).astype(BF16)
        if o % 2 == 0:
            rdma(comb.at[o], from_left.at[o], tail_send.at[2], left_sem.at[o], right).start()
        else:
            rdma(comb.at[o], from_right.at[o], tail_send.at[2], right_sem.at[o], left).start()
    for o, j in enumerate(columns):
        rdma(comb.at[o], from_left.at[o], tail_send.at[2], left_sem.at[o], right).wait_recv()
        rdma(comb.at[o], from_right.at[o], tail_send.at[2], right_sem.at[o], left).wait_recv()
        total = part[o, t].astype(F32) + from_left[o].astype(F32) + from_right[o].astype(F32)
        out[:, pl.ds(pl.multiple_of(j * CW, CW), CW)] = total.astype(BF16)

    for i in range(3):
        rdma(comb, rel, tail_send.at[i], rel_sem.at[0], right).wait_send()
    tail_copy.wait_send()

    @pl.when(c == W)
    def _():
        rdma(ubuf, u0, u0_sem.at[0], u0_sem.at[1], partner).wait_send()
        for sem, ref in enumerate((wt.at[0:15, 0], wt.at[0:8], wt.at[0:4])):
            rdma(ref, ref, ws_sem.at[sem], zsem.at[0, 0], partner).wait_send()
        rdma(wt, wt, fs_sem, fsem.at[0], partner).wait_send()

    @pl.when(c == S)
    def _():
        rdma(wblk, wt.at[0, 0, 0:16], wd_sem.at[0], wd_sem.at[1], partner).wait_send()
        rdma(pbuf.at[0:3], prec.at[0:3], p_sem.at[0], p_sem.at[1], partner).wait_send()
        rdma(arec, arec, a_sem.at[5], a_sem.at[0], partner).wait_send()
        rdma(brec, brec, b_sem.at[2], b_sem.at[0], partner).wait_send()
        rdma(rbuf.at[0:3], sin.at[0:3], r_sem.at[0], r_sem.at[1], partner).wait_send()
        rdma(sin, sin, sin_sem.at[0], sin_sem.at[1], partner).wait_send()


def solution(mesh):
    nt = mesh.shape["tp"]
    nz = mesh.shape["sp"] // (NX * NC)

    def step(
        queries, keys, values, gate_code, gate_up, gate_bias, gla_gain,
        conv_input, conv_gate, conv_taps, out_gla, out_conv,
    ):
        width = HEADS * HV
        vm, dma = pltpu.VMEM, pltpu.SemaphoreType.DMA
        quarter = ROWS // nt
        scratch = [
            vm((nz, NX, 32, 2 * width), BF16),
            vm((SEGS, width, KW), F32),
            vm((SEGS, 8, HEADS * KW), F32),
            vm((width + 16, KW), BF16),
            vm((width + 16, KW), BF16),
            vm((NX, KW + 16, KW), BF16),
            vm((NX, KW + 16, KW), BF16),
            vm((KW + 16, KW), BF16),
            vm((5, KW + 16, KW), BF16),
            vm((KW + 16, KW), BF16),
            vm((2, KW + 16, KW), BF16),
            vm((NX, KW, KW), BF16),
            vm((NX, KW, KW), BF16),
            vm((16, width), BF16),
            vm((8 + ROWS, width), F32),
            vm((ROWS, 2 * width), BF16),
            vm((16, 2 * width), BF16),
            vm((NX, KW, KW), BF16),
            vm((NCHUNK, nt, quarter, CW), BF16),
            vm((NCHUNK, quarter, CW), BF16),
            vm((NCHUNK, quarter, CW), BF16),
            vm((NCHUNK, quarter, CW), BF16),
            vm((NCHUNK, quarter, CW), BF16),
            dma((nz, NX)), dma((nz,)), dma((3,)), dma, dma((2,)),
            dma((2,)), dma((5,)), dma((6,)), dma((3,)), dma((5,)), dma((2,)), dma((2,)),
            dma((NCHUNK,)), dma((NCHUNK,)), dma((NCHUNK,)), dma((3,)),
        ]
        return pl.pallas_call(
            functools.partial(layer_kernel, nz, nt),
            out_shape=jax.ShapeDtypeStruct((quarter, 2048), BF16),
            in_specs=[pl.BlockSpec(memory_space=pltpu.VMEM)] * 12,
            out_specs=pl.BlockSpec(memory_space=pltpu.VMEM),
            scratch_shapes=scratch,
            compiler_params=pltpu.CompilerParams(collective_id=0, has_side_effects=True),
            name="layer",
        )(
            queries, keys, values, gate_code.T, gate_up, gate_bias[None], gla_gain[None],
            conv_input, conv_gate, conv_taps, out_gla.T, out_conv.T,
        )

    return jax.shard_map(
        step,
        mesh=mesh,
        in_specs=(
            P("sp", "tp"), P("sp", "tp"), P("sp", "tp"), P("sp", None), P(None, "tp"),
            P("tp"), P(), P("sp", "tp"), P("sp", "tp"), P(None, "tp"),
            P("tp", "sp"), P("tp", "sp"),
        ),
        out_specs=P(("sp", "tp"), None),
        check_vma=False,
    )
```

```python
import functools

import jax
import jax.numpy as jnp
from jax import lax
from jax.experimental import pallas as pl
from jax.experimental.pallas import tpu as pltpu
from jax.sharding import PartitionSpec as P

MESH = pl.DeviceIdType.MESH
F32, BF16 = jnp.float32, jnp.bfloat16

NX, NC = 4, 2
KW, HV, SEG = 128, 256, 64
HEADS = 2
ROWS = 256
SEGS = ROWS // SEG
NCHUNK = 8
CW = 256
W, S = 1, 0
X_ORDER = (1, 3, 2)
NEAR = (1, 2, 3)
A_SEND = (1, 2, 3, -1, -2)
B_SEND = (5, -5)
Z_SENDS = {
    0: (1, -1, 5, -5), 5: (1, -1), -5: (1, -1), -1: (1,), 1: (-1,),
    4: (1,), 6: (-1,), 7: (-1,), -6: (1,), -4: (-1,),
}
ARRIVE, RELAY, FINISH = range(3)
ROW_ORDER = (0, 1, -1, -2, 2, 5, -5, 4, -4, 6, -6, -3, 7, 3, -7, 8)
BEFORE_STATES = (
    (ARRIVE, 1), (ARRIVE, -1), (RELAY, 0), (RELAY, 1), (RELAY, -1), (ARRIVE, -2),
    (ARRIVE, 2), (ARRIVE, 5), (FINISH, 0), (ARRIVE, -5), (ARRIVE, 4), (FINISH, 1),
    (FINISH, -1), (RELAY, -2), (RELAY, 2), (RELAY, 5), (ARRIVE, 6), (ARRIVE, -4),
    (RELAY, -5), (RELAY, 4), (ARRIVE, -6), (ARRIVE, 7), (FINISH, -2), (FINISH, 2),
    (RELAY, -4), (FINISH, 5), (ARRIVE, -3), (ARRIVE, 3), (ARRIVE, 8), (FINISH, -5),
    (FINISH, 4), (RELAY, 6), (ARRIVE, -7), (RELAY, -6), (RELAY, -3), (FINISH, -4),
    (RELAY, 7), (RELAY, 3), (RELAY, 8), (RELAY, -7),
)
DONE = 4
NT = (((1,), (1,)), ((), ()))
TN = (((0,), (0,)), ((), ()))


def terms(a):
    high = a.astype(BF16).astype(F32)
    rest = a - high
    mid = rest.astype(BF16).astype(F32)
    return [high, mid, rest - mid]


def decay_rows(*decays):
    rows = [r for a in decays for r in terms(a)]
    rows.append(jnp.zeros((16 - len(rows), KW), F32))
    return jnp.concatenate(rows, axis=0).astype(BF16)


def decay_of(block, which=0):
    b = block.astype(F32)
    i = 3 * which
    return b[i : i + 1] + b[i + 1 : i + 2] + b[i + 2 : i + 3]


def chain(earlier, latter):
    return earlier[0] * latter[0], latter[0] * earlier[1] + latter[1]


def only_if(valid, pair):
    return jnp.where(valid, pair[0], 1.0), jnp.where(valid, pair[1], 0.0)


def layer_kernel(
    nz,
    nt,
    q_in, k_in, v_in, code_in, up_in, bias_in, gain_in, cin_in, cgate_in, taps_in,
    wgla_in, wconv_in,
    out,
    q, k, v, code, up, bias, gain, cin, cgate, taps,
    wt, states, through, ubuf, u0, pbuf, prec, abuf, arec, wbuf, brec, rbuf, sin,
    ctail, ext, mix, wblk, sout, part, rel, comb, from_left, from_right,
    zsem, fsem, ws_sem, fs_sem, wd_sem,
    u0_sem, p_sem, a_sem, b_sem, r_sem, sin_sem, c_sem,
    rel_sem, left_sem, right_sem, tail_send, load_sem, wload_sem,
):
    s = lax.axis_index("sp")
    t = lax.axis_index("tp")
    ns = nz * NX * NC
    c = lax.rem(s, NC)
    x = lax.rem(s // NC, NX)
    z = s // (NC * NX)

    def chip(zz, xx, cc):
        return {"sp": (zz * NX + xx) * NC + cc, "tp": t}

    def along_z(d):
        return chip(lax.rem(z + d + nz, nz), x, c)

    def along_x(d):
        return chip(z, lax.rem(x + d + NX, NX), c)

    def along_y(d):
        return {"sp": s, "tp": lax.rem(t + d + nt, nt)}

    def next_in_order(d):
        return {"sp": lax.rem(s + d + ns, ns), "tp": t}

    partner = chip(z, x, 1 - c)

    def rdma(src, dst, send, recv, dev):
        return pltpu.make_async_remote_copy(
            src_ref=src, dst_ref=dst, send_sem=send, recv_sem=recv,
            device_id=dev, device_id_type=MESH,
        )

    barrier = pltpu.get_barrier_semaphore()

    def greet(dev):
        pl.semaphore_signal(barrier, inc=1, device_id=dev, device_id_type=MESH)

    greet(partner)
    for d in (1, 2, 3):
        greet(along_x(d))
    for d in (1, -1):
        greet(along_y(d))
        greet(next_in_order(d))

    @pl.when(c == W)
    def _():
        for d in (1, 5):
            greet(along_z(d))
            greet(along_z(-d))

    @pl.when(c == S)
    def _():
        for d in NEAR:
            greet(along_z(d))
            greet(along_z(-d))

    loads = {
        name: pltpu.make_async_copy(src, dst, load_sem.at[i])
        for i, (name, src, dst) in enumerate((
            ("code", code_in, code), ("up", up_in, up), ("bias", bias_in, bias),
            ("k", k_in, k), ("v", v_in, v), ("cin", cin_in, cin),
            ("cgate", cgate_in, cgate), ("taps", taps_in, taps), ("q", q_in, q),
            ("gain", gain_in, gain),
        ))
    }
    own_rows, other_rows = slice(16 * W, 16 * W + 16), slice(16 * S, 16 * S + 16)
    width = HEADS * HV

    def weight_loads(block):
        return (
            pltpu.make_async_copy(wgla_in, block.at[:, 0:width], wload_sem.at[0]),
            pltpu.make_async_copy(wconv_in, block.at[:, width:], wload_sem.at[1]),
        )

    @pl.when(c == W)
    def _():
        for copy in weight_loads(wt.at[z, x, own_rows]):
            copy.start()

    @pl.when(c == S)
    def _():
        for copy in weight_loads(wblk):
            copy.start()

    for copy in loads.values():
        copy.start()
    for name in ("code", "up", "bias", "k", "v"):
        loads[name].wait()
    score = lax.dot_general(code[...], up[...], TN, preferred_element_type=F32) + bias[...]
    log_decay = (jnp.minimum(score, 0.0) - jnp.log1p(jnp.exp(-jnp.abs(score)))) / 16.0
    row = lax.broadcasted_iota(jnp.int32, (SEG, SEG), 0)
    col = lax.broadcasted_iota(jnp.int32, (SEG, SEG), 1)
    later = (col > row).astype(F32)
    acc = [None] * HEADS
    thr = None
    for n in range(SEGS):
        here = log_decay[n * SEG : (n + 1) * SEG]
        rest = jnp.dot(
            later, here, preferred_element_type=F32, precision=lax.Precision.HIGHEST
        )
        scaled = (k[n * SEG : (n + 1) * SEG, :].astype(F32) * jnp.exp(rest)).astype(BF16)
        seg_decay = jnp.exp(rest[0:1] + here[0:1])
        thr = seg_decay if n == 0 else thr * seg_decay
        through[n] = jnp.broadcast_to(thr, (8, HEADS * KW))
        for h in range(HEADS):
            update = lax.dot_general(
                v[n * SEG : (n + 1) * SEG, h * HV : (h + 1) * HV],
                scaled[:, h * KW : (h + 1) * KW],
                TN,
                preferred_element_type=F32,
            )
            if n == 0:
                acc[h] = update
            else:
                acc[h] = acc[h] * seg_decay[:, h * KW : (h + 1) * KW] + update
            states[n, h * HV : (h + 1) * HV, :] = acc[h]
    for h in range(HEADS):
        ubuf[h * HV : (h + 1) * HV, :] = acc[h].astype(BF16)
    ubuf[HEADS * HV :, :] = decay_rows(thr[:, :KW], thr[:, KW:])

    @pl.when(c == W)
    def _():
        for copy in weight_loads(wt.at[z, x, own_rows]):
            copy.wait()
        pl.semaphore_wait(barrier, 12)

    @pl.when(c == S)
    def _():
        for copy in weight_loads(wblk):
            copy.wait()
        pl.semaphore_wait(barrier, 14)

    tail_copy = rdma(
        cin.at[ROWS - 16 : ROWS], ctail, c_sem.at[0], c_sem.at[1], next_in_order(1)
    )

    def conv():
        loads["cgate"].wait()
        loads["taps"].wait()
        tail_copy.wait_recv()
        ext[8:, :] = cin[...].astype(F32)
        ext[0:8, :] = jnp.where(s == 0, 0.0, ctail[...].astype(F32)[8:16])
        done = taps[0:1] * ext[6 : 6 + ROWS, :]
        done = done + taps[1:2] * ext[7 : 7 + ROWS, :]
        done = done + taps[2:3] * ext[8 : 8 + ROWS, :]
        mix[:, HEADS * HV :] = (cgate[...].astype(F32) * done).astype(BF16)

    def read_out(incoming):
        loads["q"].wait()
        loads["gain"].wait()
        for h in range(HEADS):
            for n in range(SEGS):
                decay = through[n, 0:1, h * KW : (h + 1) * KW]
                state = states[n, h * HV : (h + 1) * HV, :] + decay * incoming(h)
                got = lax.dot_general(
                    q[n * SEG : (n + 1) * SEG, h * KW : (h + 1) * KW],
                    state.astype(BF16),
                    NT,
                    preferred_element_type=F32,
                )
                scale = lax.rsqrt(jnp.mean(got * got, axis=-1, keepdims=True) + 1.0)
                mix[n * SEG : (n + 1) * SEG, h * HV : (h + 1) * HV] = (
                    got * scale * gain[...]
                ).astype(BF16)

    def arrived(h):
        return jnp.concatenate([sin[2 * h], sin[2 * h + 1]], axis=0).astype(F32)

    right, left = along_y(1), along_y(-1)
    opposite, at_right, at_left = (lax.rem(t + d, nt) for d in (2, 1, 3))

    def row_at(d):
        return lax.rem(z + d + nz, nz)

    def rows_of(o):
        return [row_at(d) for d in ROW_ORDER[2 * o : 2 * o + 2]]

    def project(o):
        w = jnp.concatenate([wt[rr].reshape(CW // 2, 2 * width) for rr in rows_of(o)], axis=0)
        got = lax.dot_general(mix[...], w, NT, preferred_element_type=F32)
        part[o] = got.astype(BF16).reshape(nt, ROWS // nt, CW)
        rdma(
            part.at[o, opposite], rel.at[o], tail_send.at[0], rel_sem.at[o],
            right if o % 2 == 0 else left,
        ).start()

    def send_direct(o):
        if o % 2 == 0:
            rdma(
                part.at[o, at_left], from_right.at[o], tail_send.at[1],
                right_sem.at[o], left,
            ).start()
        else:
            rdma(
                part.at[o, at_right], from_left.at[o], tail_send.at[1],
                left_sem.at[o], right,
            ).start()

    def combine(o):
        to = right if o % 2 == 0 else left
        rdma(part.at[o, 0], rel.at[o], tail_send.at[0], rel_sem.at[o], to).wait_recv()
        mine = part[o, at_right if o % 2 == 0 else at_left]
        comb[o] = (rel[o].astype(F32) + mine.astype(F32)).astype(BF16)
        if o % 2 == 0:
            rdma(comb.at[o], from_left.at[o], tail_send.at[2], left_sem.at[o], right).start()
        else:
            rdma(comb.at[o], from_right.at[o], tail_send.at[2], right_sem.at[o], left).start()

    def conclude(o):
        rdma(comb.at[o], from_left.at[o], tail_send.at[2], left_sem.at[o], right).wait_recv()
        rdma(comb.at[o], from_right.at[o], tail_send.at[2], right_sem.at[o], left).wait_recv()
        total = part[o, t].astype(F32) + from_left[o].astype(F32) + from_right[o].astype(F32)
        for i, rr in enumerate(rows_of(o)):
            half = CW // 2
            out[:, pl.ds(pl.multiple_of(rr * half, half), half)] = total[
                :, i * half : (i + 1) * half
            ].astype(BF16)

    def send_block(rr, xx, sem, dev):
        block = wt.at[rr, xx]
        rdma(block, block, ws_sem.at[sem], zsem.at[rr, xx], dev).start()

    def wait_block(rr, xx):
        block = wt.at[rr, xx]
        rdma(block, block, ws_sem.at[0], zsem.at[rr, xx], partner).wait_recv()

    def x_at(d):
        return lax.rem(x + d, NX)

    def arrive(d):
        if d != 0:
            wait_block(row_at(d), x)
        for to in Z_SENDS.get(d, ()):
            send_block(row_at(d), x, 0, along_z(to))
        for to in (1, 3):
            send_block(row_at(d), x, 1, along_x(to))

    def relay(d):
        near = 3 if d <= 0 else 1
        wait_block(row_at(d), x_at(near))
        send_block(row_at(d), x_at(near), 2, along_x(4 - near))

    def finish(d):
        far = 1 if d <= 0 else 3
        wait_block(row_at(d), x_at(far))
        wait_block(row_at(d), x_at(2))
        rr = row_at(d)
        rdma(wt.at[rr], wt.at[rr], fs_sem, fsem.at[rr], partner).start()

    @pl.when(c == W)
    def _():
        rdma(ubuf, u0, u0_sem.at[0], u0_sem.at[1], partner).start()
        loads["cin"].wait()
        tail_copy.start()
        rdma(wblk, wt.at[z, x, other_rows], wd_sem.at[0], wd_sem.at[1], partner).wait_recv()
        arrive(0)
        conv()
        for what, d in BEFORE_STATES:
            (arrive, relay, finish)[what](d)
        rdma(sin, sin, sin_sem.at[0], sin_sem.at[1], partner).wait_recv()
        read_out(arrived)
        for o in range(DONE):
            project(o)
        for o in range(DONE):
            send_direct(o)
        for o in range(DONE, NCHUNK):
            for d in ROW_ORDER[max(2 * o, 9) : 2 * o + 2]:
                finish(d)
            project(o)
        for o in range(DONE, NCHUNK):
            send_direct(o)

    @pl.when(c == S)
    def _():
        rdma(wblk, wt.at[z, x, other_rows], wd_sem.at[0], wd_sem.at[1], partner).start()
        loads["cin"].wait()
        tail_copy.start()
        rdma(ubuf, u0, u0_sem.at[0], u0_sem.at[1], partner).wait_recv()

        def theirs(h, lo, hi):
            return (
                decay_of(u0[HEADS * HV :, :], h),
                u0[h * HV + lo : h * HV + hi, :].astype(F32),
            )

        def ours(h, lo, hi):
            return thr[:, h * KW : (h + 1) * KW], acc[h][lo:hi]

        first, second = (theirs, ours) if S == 1 else (ours, theirs)
        for i in range(NX):
            part_of = (i // 2, (i % 2) * KW, (i % 2 + 1) * KW)
            both = chain(first(*part_of), second(*part_of))
            pbuf[i, 0:KW, :] = both[1].astype(BF16)
            pbuf[i, KW:, :] = decay_rows(both[0])
        for j, d in enumerate((1, 3, 2)):
            rdma(
                pbuf.at[lax.rem(x + d, NX)], prec.at[x],
                p_sem.at[0], p_sem.at[1 + d], along_x(d),
            ).start()
        prec[x] = pbuf[x]
        for d in (1, 2, 3):
            rdma(
                pbuf.at[0], prec.at[lax.rem(x - d + NX, NX)],
                p_sem.at[0], p_sem.at[1 + d], along_x(d),
            ).wait_recv()

        def pair_in(ref, i):
            return decay_of(ref[i, KW:, :]), ref[i, 0:KW, :].astype(F32)

        chips = [pair_in(prec, i) for i in range(NX)]
        plane = chips[0]
        for i in range(1, NX):
            plane = chain(plane, chips[i])
        abuf[0:KW, :] = plane[1].astype(BF16)
        abuf[KW:, :] = decay_rows(plane[0])
        for j, d in enumerate(A_SEND):
            rdma(abuf, arec.at[j], a_sem.at[5], a_sem.at[j], along_z(d)).start()
        conv()
        for j, d in enumerate(A_SEND):
            rdma(abuf, arec.at[j], a_sem.at[5], a_sem.at[j], along_z(d)).wait_recv()
        back1, back2, back3, ahead1, ahead2 = (pair_in(arec, j) for j in range(5))
        inner = z <= nz - 6
        window = chain(
            only_if(inner & (z >= 2), back2), only_if(inner & (z >= 1), back1)
        )
        window = chain(window, only_if(inner, plane))
        window = chain(window, only_if(inner | (z == nz - 1), ahead1))
        window = chain(window, only_if(inner | (z >= nz - 2), ahead2))
        wider = chain(only_if(inner & (z >= 3), back3), window)
        for j, (decay, state) in enumerate((wider, window)):
            wbuf[j, 0:KW, :] = state.astype(BF16)
            wbuf[j, KW:, :] = decay_rows(decay)
        for j, d in enumerate(B_SEND):
            rdma(wbuf.at[j], brec.at[j], b_sem.at[2], b_sem.at[j], along_z(d)).start()
        oldest = chain(only_if(z >= nz - 1, ahead1), only_if(z >= nz - 2, ahead2))
        newest = chain(only_if(z >= 2, back2), only_if(z >= 1, back1))
        for j, d in enumerate(B_SEND):
            rdma(wbuf.at[j], brec.at[j], b_sem.at[2], b_sem.at[j], along_z(d)).wait_recv()
        before = chain(oldest, only_if(z >= 9, pair_in(brec, 1)))
        before = chain(before, only_if(z >= 3, pair_in(brec, 0)))
        before = chain(before, newest)
        run = before[1]
        for i in range(NX):
            rbuf[i] = run.astype(BF16)
            if i < NX - 1:
                run = chips[i][0] * run + chips[i][1]
        for d in (1, 3, 2):
            rdma(
                rbuf.at[lax.rem(x + d, NX)], sin.at[x],
                r_sem.at[0], r_sem.at[1 + d], along_x(d),
            ).start()
        sin[x] = rbuf[x]
        for d in (1, 2, 3):
            rdma(
                rbuf.at[0], sin.at[lax.rem(x - d + NX, NX)],
                r_sem.at[0], r_sem.at[1 + d], along_x(d),
            ).wait_recv()

        def after_first(h):
            decay, update = first(h, 0, HV)
            return decay * arrived(h) + update

        if S == 1:
            rdma(sin, sin, sin_sem.at[0], sin_sem.at[1], partner).start()
        else:
            for h in range(HEADS):
                sout[2 * h : 2 * h + 2] = after_first(h).astype(BF16).reshape(2, KW, KW)
            rdma(sout, sin, sin_sem.at[0], sin_sem.at[1], partner).start()
        read_out(after_first if S == 1 else arrived)
        for o in range(NCHUNK):
            for rr in rows_of(o):
                rdma(wt.at[rr], wt.at[rr], fs_sem, fsem.at[rr], partner).wait_recv()
            project(o)
        for o in range(NCHUNK):
            send_direct(o)

    for o in range(NCHUNK):
        combine(o)
    for o in range(NCHUNK):
        conclude(o)
    for i in range(3):
        rdma(comb, rel, tail_send.at[i], rel_sem.at[0], right).wait_send()
    tail_copy.wait_send()

    @pl.when(c == W)
    def _():
        rdma(ubuf, u0, u0_sem.at[0], u0_sem.at[1], partner).wait_send()
        for sem, ref in enumerate((wt.at[0:15, 0], wt.at[0:8], wt.at[0:4])):
            rdma(ref, ref, ws_sem.at[sem], zsem.at[0, 0], partner).wait_send()
        rdma(wt, wt, fs_sem, fsem.at[0], partner).wait_send()

    @pl.when(c == S)
    def _():
        rdma(wblk, wt.at[0, 0, 0:16], wd_sem.at[0], wd_sem.at[1], partner).wait_send()
        rdma(pbuf.at[0:3], prec.at[0:3], p_sem.at[0], p_sem.at[1], partner).wait_send()
        rdma(arec, arec, a_sem.at[5], a_sem.at[0], partner).wait_send()
        rdma(brec, brec, b_sem.at[2], b_sem.at[0], partner).wait_send()
        rdma(rbuf.at[0:3], sin.at[0:3], r_sem.at[0], r_sem.at[1], partner).wait_send()
        rdma(sin, sin, sin_sem.at[0], sin_sem.at[1], partner).wait_send()


def solution(mesh):
    nt = mesh.shape["tp"]
    nz = mesh.shape["sp"] // (NX * NC)

    def step(
        queries, keys, values, gate_code, gate_up, gate_bias, gla_gain,
        conv_input, conv_gate, conv_taps, out_gla, out_conv,
    ):
        width = HEADS * HV
        vm, dma = pltpu.VMEM, pltpu.SemaphoreType.DMA
        quarter = ROWS // nt
        scratch = [
            vm((ROWS, HEADS * KW), BF16),
            vm((ROWS, HEADS * KW), BF16),
            vm((ROWS, width), BF16),
            vm((32, ROWS), BF16),
            vm((32, HEADS * KW), BF16),
            vm((1, HEADS * KW), F32),
            vm((1, HV), F32),
            vm((ROWS, width), BF16),
            vm((ROWS, width), BF16),
            vm((3, width), F32),
            vm((nz, NX, 32, 2 * width), BF16),
            vm((SEGS, width, KW), F32),
            vm((SEGS, 8, HEADS * KW), F32),
            vm((width + 16, KW), BF16),
            vm((width + 16, KW), BF16),
            vm((NX, KW + 16, KW), BF16),
            vm((NX, KW + 16, KW), BF16),
            vm((KW + 16, KW), BF16),
            vm((5, KW + 16, KW), BF16),
            vm((2, KW + 16, KW), BF16),
            vm((2, KW + 16, KW), BF16),
            vm((NX, KW, KW), BF16),
            vm((NX, KW, KW), BF16),
            vm((16, width), BF16),
            vm((8 + ROWS, width), F32),
            vm((ROWS, 2 * width), BF16),
            vm((16, 2 * width), BF16),
            vm((NX, KW, KW), BF16),
            vm((NCHUNK, nt, quarter, CW), BF16),
            vm((NCHUNK, quarter, CW), BF16),
            vm((NCHUNK, quarter, CW), BF16),
            vm((NCHUNK, quarter, CW), BF16),
            vm((NCHUNK, quarter, CW), BF16),
            dma((nz, NX)), dma((nz,)), dma((3,)), dma, dma((2,)),
            dma((2,)), dma((5,)), dma((6,)), dma((3,)), dma((5,)), dma((2,)), dma((2,)),
            dma((NCHUNK,)), dma((NCHUNK,)), dma((NCHUNK,)), dma((3,)), dma((10,)), dma((2,)),
        ]
        return pl.pallas_call(
            functools.partial(layer_kernel, nz, nt),
            out_shape=jax.ShapeDtypeStruct((quarter, 2048), BF16),
            in_specs=[pl.BlockSpec(memory_space=pl.ANY)] * 12,
            out_specs=pl.BlockSpec(memory_space=pltpu.VMEM),
            scratch_shapes=scratch,
            compiler_params=pltpu.CompilerParams(collective_id=0, has_side_effects=True),
            name="layer",
        )(
            queries, keys, values, gate_code.T, gate_up, gate_bias[None], gla_gain[None],
            conv_input, conv_gate, conv_taps, out_gla.T, out_conv.T,
        )

    return jax.shard_map(
        step,
        mesh=mesh,
        in_specs=(
            P("sp", "tp"), P("sp", "tp"), P("sp", "tp"), P("sp", None), P(None, "tp"),
            P("tp"), P(), P("sp", "tp"), P("sp", "tp"), P(None, "tp"),
            P("tp", "sp"), P("tp", "sp"),
        ),
        out_specs=P(("sp", "tp"), None),
        check_vma=False,
    )
```

```python
import functools

import jax
import jax.numpy as jnp
from jax import lax
from jax.experimental import pallas as pl
from jax.experimental.pallas import tpu as pltpu
from jax.sharding import PartitionSpec as P

MESH = pl.DeviceIdType.MESH
F32, BF16 = jnp.float32, jnp.bfloat16

NX, NC = 4, 2
KW, HV, SEG = 128, 256, 64
HEADS = 2
ROWS = 256
SEGS = ROWS // SEG
NCHUNK = 8
CW = 256
W, S = 1, 0
X_ORDER = (1, 3, 2)
NEAR = (1, 2, 3)
W_GREETINGS, S_GREETINGS = 12, 14
A_SEND = (3, -2, 2, -1, 1)
B_SEND = (5, -5)
Z_SENDS = {
    0: (1, -1, 4, -4), 1: (-1,), -1: (1,), 4: (1, -1), -4: (1, -1),
    5: (-1,), -5: (1,), 6: (-1,), -6: (1,), 7: (-1,),
}
ARRIVE, RELAY, FINISH, CONV = range(4)
ROW_ORDER = (0, -1, 1, 4, -2, -4, 2, 5, -5, -6, 6, -3, 3, 7, 8, -7)
BEFORE_STATES = (
    (ARRIVE, 1), (ARRIVE, -1), (RELAY, 0), (ARRIVE, 4), (RELAY, 1), (RELAY, -1),
    (CONV, 0), (ARRIVE, -2), (ARRIVE, 2), (ARRIVE, -4), (RELAY, 4), (FINISH, 0),
    (ARRIVE, 5), (ARRIVE, -3), (FINISH, -1), (FINISH, 1), (RELAY, -2), (ARRIVE, -5),
    (RELAY, -4), (RELAY, 2), (ARRIVE, 6), (RELAY, 5), (FINISH, 4), (ARRIVE, -6),
    (ARRIVE, 3), (FINISH, -2), (RELAY, -5), (ARRIVE, 7), (ARRIVE, -7), (FINISH, -4),
    (FINISH, 2), (RELAY, -6), (FINISH, 5), (RELAY, -3), (ARRIVE, 8), (RELAY, 6),
    (RELAY, 3), (FINISH, -5), (RELAY, 7), (RELAY, -7), (RELAY, 8),
)
W_COMBINES = ((), (), (), (), (), (), (), tuple(range(8)))
S_COMBINES = ((), (), (), (0,), (), (1,), (), (2, 3, 4, 5, 6, 7))
LAST_ROWS = ((-6, 6), (-3, 3), (7,), (8, -7), (), (), (), ())
NT = (((1,), (1,)), ((), ()))
TN = (((0,), (0,)), ((), ()))


def terms(a):
    high = a.astype(BF16).astype(F32)
    rest = a - high
    mid = rest.astype(BF16).astype(F32)
    return [high, mid, rest - mid]


def decay_rows(*decays):
    rows = [r for a in decays for r in terms(a)]
    rows.append(jnp.zeros((16 - len(rows), KW), F32))
    return jnp.concatenate(rows, axis=0).astype(BF16)


def decay_of(block, which=0):
    b = block.astype(F32)
    i = 3 * which
    return b[i : i + 1] + b[i + 1 : i + 2] + b[i + 2 : i + 3]


def chain(earlier, latter):
    return earlier[0] * latter[0], latter[0] * earlier[1] + latter[1]


def only_if(valid, pair):
    return jnp.where(valid, pair[0], 1.0), jnp.where(valid, pair[1], 0.0)


def layer_kernel(
    nz,
    nt,
    q_in, k_in, v_in, code_in, up_in, bias_in, gain_in, cin_in, cgate_in, taps_in,
    wgla_in, wconv_in,
    out,
    q, k, v, code, up, bias, gain, cin, cgate, taps,
    wt, states, through, ubuf, u0, pbuf, prec, abuf, arec, wbuf, brec, rbuf, sin,
    ctail, ext, mix, wblk, sout, part, rel, comb, from_left, from_right,
    zsem, fsem, ws_sem, fs_sem, wd_sem,
    u0_sem, p_sem, a_sem, b_sem, r_sem, sin_sem, c_sem,
    rel_sem, left_sem, right_sem, tail_send, load_sem, wload_sem,
):
    s = lax.axis_index("sp")
    t = lax.axis_index("tp")
    ns = nz * NX * NC
    c = lax.rem(s, NC)
    x = lax.rem(s // NC, NX)
    z = s // (NC * NX)

    def chip(zz, xx, cc):
        return {"sp": (zz * NX + xx) * NC + cc, "tp": t}

    def along_z(d):
        return chip(lax.rem(z + d + nz, nz), x, c)

    def along_x(d):
        return chip(z, lax.rem(x + d + NX, NX), c)

    def along_y(d):
        return {"sp": s, "tp": lax.rem(t + d + nt, nt)}

    def next_in_order(d):
        return {"sp": lax.rem(s + d + ns, ns), "tp": t}

    partner = chip(z, x, 1 - c)

    def rdma(src, dst, send, recv, dev):
        return pltpu.make_async_remote_copy(
            src_ref=src, dst_ref=dst, send_sem=send, recv_sem=recv,
            device_id=dev, device_id_type=MESH,
        )

    barrier = pltpu.get_barrier_semaphore()

    def greet(dev):
        pl.semaphore_signal(barrier, inc=1, device_id=dev, device_id_type=MESH)

    greet(partner)
    for d in (1, 2, 3):
        greet(along_x(d))
    for d in (1, -1):
        greet(along_y(d))
        greet(next_in_order(d))

    @pl.when(c == W)
    def _():
        for d in (1, 4):
            greet(along_z(d))
            greet(along_z(-d))

    @pl.when(c == S)
    def _():
        for d in NEAR:
            greet(along_z(d))
            greet(along_z(-d))

    loads = {
        name: pltpu.make_async_copy(src, dst, load_sem.at[i])
        for i, (name, src, dst) in enumerate((
            ("code", code_in, code), ("up", up_in, up), ("bias", bias_in, bias),
            ("k", k_in, k), ("v", v_in, v), ("cin", cin_in, cin),
            ("cgate", cgate_in, cgate), ("taps", taps_in, taps), ("q", q_in, q),
            ("gain", gain_in, gain),
        ))
    }
    own_rows, other_rows = slice(16 * W, 16 * W + 16), slice(16 * S, 16 * S + 16)
    width = HEADS * HV

    def weight_loads(block):
        return (
            pltpu.make_async_copy(wgla_in, block.at[:, 0:width], wload_sem.at[0]),
            pltpu.make_async_copy(wconv_in, block.at[:, width:], wload_sem.at[1]),
        )

    @pl.when(c == W)
    def _():
        for copy in weight_loads(wt.at[z, x, own_rows]):
            copy.start()

    @pl.when(c == S)
    def _():
        for copy in weight_loads(wblk):
            copy.start()

    for copy in loads.values():
        copy.start()
    @pl.when(c == S)
    def _():
        for copy in weight_loads(wblk):
            copy.wait()
        pl.semaphore_wait(barrier, S_GREETINGS)
        rdma(wblk, wt.at[z, x, other_rows], wd_sem.at[0], wd_sem.at[1], partner).start()

    for name in ("code", "up", "bias"):
        loads[name].wait()
    score = lax.dot_general(code[...], up[...], TN, preferred_element_type=F32) + bias[...]
    log_decay = (jnp.minimum(score, 0.0) - jnp.log1p(jnp.exp(-jnp.abs(score)))) / 16.0
    row = lax.broadcasted_iota(jnp.int32, (SEG, SEG), 0)
    col = lax.broadcasted_iota(jnp.int32, (SEG, SEG), 1)
    later = (col > row).astype(F32)
    acc = [None] * HEADS
    thr = None
    for n in range(SEGS):
        here = log_decay[n * SEG : (n + 1) * SEG]
        rest = jnp.dot(
            later, here, preferred_element_type=F32, precision=lax.Precision.HIGHEST
        )
        if n == 0:
            loads["k"].wait()
            loads["v"].wait()
        scaled = (k[n * SEG : (n + 1) * SEG, :].astype(F32) * jnp.exp(rest)).astype(BF16)
        seg_decay = jnp.exp(rest[0:1] + here[0:1])
        thr = seg_decay if n == 0 else thr * seg_decay
        through[n] = jnp.broadcast_to(thr, (8, HEADS * KW))
        for h in range(HEADS):
            update = lax.dot_general(
                v[n * SEG : (n + 1) * SEG, h * HV : (h + 1) * HV],
                scaled[:, h * KW : (h + 1) * KW],
                TN,
                preferred_element_type=F32,
            )
            if n == 0:
                acc[h] = update
            else:
                acc[h] = acc[h] * seg_decay[:, h * KW : (h + 1) * KW] + update
            states[n, h * HV : (h + 1) * HV, :] = acc[h]
    for h in range(HEADS):
        ubuf[h * HV : (h + 1) * HV, :] = acc[h].astype(BF16)
    ubuf[HEADS * HV :, :] = decay_rows(thr[:, :KW], thr[:, KW:])

    @pl.when(c == W)
    def _():
        for copy in weight_loads(wt.at[z, x, own_rows]):
            copy.wait()
        pl.semaphore_wait(barrier, W_GREETINGS)

    tail_copy = rdma(
        cin.at[ROWS - 16 : ROWS], ctail, c_sem.at[0], c_sem.at[1], next_in_order(1)
    )

    def conv():
        loads["cgate"].wait()
        loads["taps"].wait()
        tail_copy.wait_recv()
        ext[8:, :] = cin[...].astype(F32)
        ext[0:8, :] = jnp.where(s == 0, 0.0, ctail[...].astype(F32)[8:16])
        done = taps[0:1] * ext[6 : 6 + ROWS, :]
        done = done + taps[1:2] * ext[7 : 7 + ROWS, :]
        done = done + taps[2:3] * ext[8 : 8 + ROWS, :]
        mix[:, HEADS * HV :] = (cgate[...].astype(F32) * done).astype(BF16)

    def read_out(incoming):
        loads["q"].wait()
        loads["gain"].wait()
        for h in range(HEADS):
            for n in range(SEGS):
                decay = through[n, 0:1, h * KW : (h + 1) * KW]
                state = states[n, h * HV : (h + 1) * HV, :] + decay * incoming(h)
                got = lax.dot_general(
                    q[n * SEG : (n + 1) * SEG, h * KW : (h + 1) * KW],
                    state.astype(BF16),
                    NT,
                    preferred_element_type=F32,
                )
                scale = lax.rsqrt(jnp.mean(got * got, axis=-1, keepdims=True) + 1.0)
                mix[n * SEG : (n + 1) * SEG, h * HV : (h + 1) * HV] = (
                    got * scale * gain[...]
                ).astype(BF16)

    def arrived(h):
        return jnp.concatenate([sin[2 * h], sin[2 * h + 1]], axis=0).astype(F32)

    right, left = along_y(1), along_y(-1)
    opposite, at_right, at_left = (lax.rem(t + d, nt) for d in (2, 1, 3))

    def row_at(d):
        return lax.rem(z + d + nz, nz)

    def rows_of(o):
        return [row_at(d) for d in ROW_ORDER[2 * o : 2 * o + 2]]

    def project(o):
        w = jnp.concatenate([wt[rr].reshape(CW // 2, 2 * width) for rr in rows_of(o)], axis=0)
        got = lax.dot_general(mix[...], w, NT, preferred_element_type=F32)
        part[o] = got.astype(BF16).reshape(nt, ROWS // nt, CW)
        rdma(
            part.at[o, opposite], rel.at[o], tail_send.at[0], rel_sem.at[o],
            right if o % 2 == 0 else left,
        ).start()

    def send_direct(o):
        if o % 2 == 0:
            rdma(
                part.at[o, at_left], from_right.at[o], tail_send.at[1],
                right_sem.at[o], left,
            ).start()
        else:
            rdma(
                part.at[o, at_right], from_left.at[o], tail_send.at[1],
                left_sem.at[o], right,
            ).start()

    def combine(o):
        to = right if o % 2 == 0 else left
        rdma(part.at[o, 0], rel.at[o], tail_send.at[0], rel_sem.at[o], to).wait_recv()
        mine = part[o, at_right if o % 2 == 0 else at_left]
        comb[o] = (rel[o].astype(F32) + mine.astype(F32)).astype(BF16)
        if o % 2 == 0:
            rdma(comb.at[o], from_left.at[o], tail_send.at[2], left_sem.at[o], right).start()
        else:
            rdma(comb.at[o], from_right.at[o], tail_send.at[2], right_sem.at[o], left).start()

    def conclude(o):
        rdma(comb.at[o], from_left.at[o], tail_send.at[2], left_sem.at[o], right).wait_recv()
        rdma(comb.at[o], from_right.at[o], tail_send.at[2], right_sem.at[o], left).wait_recv()
        total = part[o, t].astype(F32) + from_left[o].astype(F32) + from_right[o].astype(F32)
        for i, rr in enumerate(rows_of(o)):
            half = CW // 2
            out[:, pl.ds(pl.multiple_of(rr * half, half), half)] = total[
                :, i * half : (i + 1) * half
            ].astype(BF16)

    def send_block(rr, xx, sem, dev):
        block = wt.at[rr, xx]
        rdma(block, block, ws_sem.at[sem], zsem.at[rr, xx], dev).start()

    def wait_block(rr, xx):
        block = wt.at[rr, xx]
        rdma(block, block, ws_sem.at[0], zsem.at[rr, xx], partner).wait_recv()

    def x_at(d):
        return lax.rem(x + d, NX)

    def arrive(d):
        if d != 0:
            wait_block(row_at(d), x)
        for to in Z_SENDS.get(d, ()):
            send_block(row_at(d), x, 0, along_z(to))
        for to in (1, 3):
            send_block(row_at(d), x, 1, along_x(to))

    def relay(d):
        near = 3 if d <= 0 else 1
        wait_block(row_at(d), x_at(near))
        send_block(row_at(d), x_at(near), 2, along_x(4 - near))

    def finish(d):
        far = 1 if d <= 0 else 3
        wait_block(row_at(d), x_at(far))
        wait_block(row_at(d), x_at(2))
        rr = row_at(d)
        rdma(wt.at[rr], wt.at[rr], fs_sem, fsem.at[rr], partner).start()

    @pl.when(c == W)
    def _():
        rdma(ubuf, u0, u0_sem.at[0], u0_sem.at[1], partner).start()
        loads["cin"].wait()
        tail_copy.start()
        rdma(wblk, wt.at[z, x, other_rows], wd_sem.at[0], wd_sem.at[1], partner).wait_recv()
        arrive(0)
        for what, d in BEFORE_STATES:
            (arrive, relay, finish, lambda _: conv())[what](d)
        rdma(sin, sin, sin_sem.at[0], sin_sem.at[1], partner).wait_recv()
        read_out(arrived)
        for o in range(NCHUNK):
            project(o)
            for d in LAST_ROWS[o]:
                finish(d)
            send_direct(o)
            for i in W_COMBINES[o]:
                combine(i)

    @pl.when(c == S)
    def _():
        loads["cin"].wait()
        tail_copy.start()
        rdma(ubuf, u0, u0_sem.at[0], u0_sem.at[1], partner).wait_recv()

        def theirs(h, lo, hi):
            return (
                decay_of(u0[HEADS * HV :, :], h),
                u0[h * HV + lo : h * HV + hi, :].astype(F32),
            )

        def ours(h, lo, hi):
            return thr[:, h * KW : (h + 1) * KW], acc[h][lo:hi]

        first, second = (theirs, ours) if S == 1 else (ours, theirs)
        for i in range(NX):
            part_of = (i // 2, (i % 2) * KW, (i % 2 + 1) * KW)
            both = chain(first(*part_of), second(*part_of))
            pbuf[i, 0:KW, :] = both[1].astype(BF16)
            pbuf[i, KW:, :] = decay_rows(both[0])
        for d in (2, 1, 3):
            rdma(
                pbuf.at[lax.rem(x + d, NX)], prec.at[x],
                p_sem.at[0], p_sem.at[1 + d], along_x(d),
            ).start()
        prec[x] = pbuf[x]
        for d in (1, 2, 3):
            rdma(
                pbuf.at[0], prec.at[lax.rem(x - d + NX, NX)],
                p_sem.at[0], p_sem.at[1 + d], along_x(d),
            ).wait_recv()

        def pair_in(ref, i):
            return decay_of(ref[i, KW:, :]), ref[i, 0:KW, :].astype(F32)

        chips = [pair_in(prec, i) for i in range(NX)]
        plane = chips[0]
        for i in range(1, NX):
            plane = chain(plane, chips[i])
        abuf[0:KW, :] = plane[1].astype(BF16)
        abuf[KW:, :] = decay_rows(plane[0])
        for j, d in enumerate(A_SEND):
            rdma(abuf, arec.at[j], a_sem.at[5], a_sem.at[j], along_z(d)).start()
        conv()
        for j, d in enumerate(A_SEND):
            rdma(abuf, arec.at[j], a_sem.at[5], a_sem.at[j], along_z(d)).wait_recv()
        back3, ahead2, back2, ahead1, back1 = (pair_in(arec, j) for j in range(5))
        inner = z <= nz - 6
        window = chain(
            only_if(inner & (z >= 2), back2), only_if(inner & (z >= 1), back1)
        )
        window = chain(window, only_if(inner, plane))
        window = chain(window, only_if(inner | (z == nz - 1), ahead1))
        window = chain(window, only_if(inner | (z >= nz - 2), ahead2))
        wider = chain(only_if(inner & (z >= 3), back3), window)
        for j, (decay, state) in enumerate((wider, window)):
            wbuf[j, 0:KW, :] = state.astype(BF16)
            wbuf[j, KW:, :] = decay_rows(decay)
        for j, d in enumerate(B_SEND):
            rdma(wbuf.at[j], brec.at[j], b_sem.at[2], b_sem.at[j], along_z(d)).start()
        oldest = chain(only_if(z >= nz - 1, ahead1), only_if(z >= nz - 2, ahead2))
        newest = chain(only_if(z >= 2, back2), only_if(z >= 1, back1))
        for j, d in enumerate(B_SEND):
            rdma(wbuf.at[j], brec.at[j], b_sem.at[2], b_sem.at[j], along_z(d)).wait_recv()
        before = chain(oldest, only_if(z >= 9, pair_in(brec, 1)))
        before = chain(before, only_if(z >= 3, pair_in(brec, 0)))
        before = chain(before, newest)
        run = before[1]
        for i in range(NX):
            rbuf[i] = run.astype(BF16)
            if i < NX - 1:
                run = chips[i][0] * run + chips[i][1]
        for d in (2, 1, 3):
            rdma(
                rbuf.at[lax.rem(x + d, NX)], sin.at[x],
                r_sem.at[0], r_sem.at[1 + d], along_x(d),
            ).start()
        sin[x] = rbuf[x]
        for d in (1, 2, 3):
            rdma(
                rbuf.at[0], sin.at[lax.rem(x - d + NX, NX)],
                r_sem.at[0], r_sem.at[1 + d], along_x(d),
            ).wait_recv()

        def after_first(h):
            decay, update = first(h, 0, HV)
            return decay * arrived(h) + update

        if S == 1:
            rdma(sin, sin, sin_sem.at[0], sin_sem.at[1], partner).start()
        else:
            for h in range(HEADS):
                sout[2 * h : 2 * h + 2] = after_first(h).astype(BF16).reshape(2, KW, KW)
            rdma(sout, sin, sin_sem.at[0], sin_sem.at[1], partner).start()
        read_out(after_first if S == 1 else arrived)
        for o in range(NCHUNK):
            for rr in rows_of(o):
                rdma(wt.at[rr], wt.at[rr], fs_sem, fsem.at[rr], partner).wait_recv()
            project(o)
            send_direct(o)
            for i in S_COMBINES[o]:
                combine(i)

    for o in range(NCHUNK):
        conclude(o)
    for i in range(3):
        rdma(comb, rel, tail_send.at[i], rel_sem.at[0], right).wait_send()
    tail_copy.wait_send()

    @pl.when(c == W)
    def _():
        rdma(ubuf, u0, u0_sem.at[0], u0_sem.at[1], partner).wait_send()
        for sem, ref in enumerate((wt.at[0:15, 0], wt.at[0:8], wt.at[0:4])):
            rdma(ref, ref, ws_sem.at[sem], zsem.at[0, 0], partner).wait_send()
        rdma(wt, wt, fs_sem, fsem.at[0], partner).wait_send()

    @pl.when(c == S)
    def _():
        rdma(wblk, wt.at[0, 0, 0:16], wd_sem.at[0], wd_sem.at[1], partner).wait_send()
        rdma(pbuf.at[0:3], prec.at[0:3], p_sem.at[0], p_sem.at[1], partner).wait_send()
        rdma(arec, arec, a_sem.at[5], a_sem.at[0], partner).wait_send()
        rdma(brec, brec, b_sem.at[2], b_sem.at[0], partner).wait_send()
        rdma(rbuf.at[0:3], sin.at[0:3], r_sem.at[0], r_sem.at[1], partner).wait_send()
        rdma(sin, sin, sin_sem.at[0], sin_sem.at[1], partner).wait_send()


def solution(mesh):
    nt = mesh.shape["tp"]
    nz = mesh.shape["sp"] // (NX * NC)

    def step(
        queries, keys, values, gate_code, gate_up, gate_bias, gla_gain,
        conv_input, conv_gate, conv_taps, out_gla, out_conv,
    ):
        width = HEADS * HV
        vm, dma = pltpu.VMEM, pltpu.SemaphoreType.DMA
        quarter = ROWS // nt
        scratch = [
            vm((ROWS, HEADS * KW), BF16),
            vm((ROWS, HEADS * KW), BF16),
            vm((ROWS, width), BF16),
            vm((32, ROWS), BF16),
            vm((32, HEADS * KW), BF16),
            vm((1, HEADS * KW), F32),
            vm((1, HV), F32),
            vm((ROWS, width), BF16),
            vm((ROWS, width), BF16),
            vm((3, width), F32),
            vm((nz, NX, 32, 2 * width), BF16),
            vm((SEGS, width, KW), F32),
            vm((SEGS, 8, HEADS * KW), F32),
            vm((width + 16, KW), BF16),
            vm((width + 16, KW), BF16),
            vm((NX, KW + 16, KW), BF16),
            vm((NX, KW + 16, KW), BF16),
            vm((KW + 16, KW), BF16),
            vm((5, KW + 16, KW), BF16),
            vm((2, KW + 16, KW), BF16),
            vm((2, KW + 16, KW), BF16),
            vm((NX, KW, KW), BF16),
            vm((NX, KW, KW), BF16),
            vm((16, width), BF16),
            vm((8 + ROWS, width), F32),
            vm((ROWS, 2 * width), BF16),
            vm((16, 2 * width), BF16),
            vm((NX, KW, KW), BF16),
            vm((NCHUNK, nt, quarter, CW), BF16),
            vm((NCHUNK, quarter, CW), BF16),
            vm((NCHUNK, quarter, CW), BF16),
            vm((NCHUNK, quarter, CW), BF16),
            vm((NCHUNK, quarter, CW), BF16),
            dma((nz, NX)), dma((nz,)), dma((3,)), dma, dma((2,)),
            dma((2,)), dma((5,)), dma((6,)), dma((3,)), dma((5,)), dma((2,)), dma((2,)),
            dma((NCHUNK,)), dma((NCHUNK,)), dma((NCHUNK,)), dma((3,)), dma((10,)), dma((2,)),
        ]
        return pl.pallas_call(
            functools.partial(layer_kernel, nz, nt),
            out_shape=pltpu.VMEM((quarter, 2048), BF16),
            in_specs=[pl.BlockSpec(memory_space=pl.ANY)] * 12,
            out_specs=pl.BlockSpec(memory_space=pltpu.VMEM),
            scratch_shapes=scratch,
            compiler_params=pltpu.CompilerParams(collective_id=0, has_side_effects=True),
            name="layer",
        )(
            queries, keys, values, gate_code.T, gate_up, gate_bias[None], gla_gain[None],
            conv_input, conv_gate, conv_taps, out_gla.T, out_conv.T,
        )

    return jax.shard_map(
        step,
        mesh=mesh,
        in_specs=(
            P("sp", "tp"), P("sp", "tp"), P("sp", "tp"), P("sp", None), P(None, "tp"),
            P("tp"), P(), P("sp", "tp"), P("sp", "tp"), P(None, "tp"),
            P("tp", "sp"), P("tp", "sp"),
        ),
        out_specs=P(("sp", "tp"), None),
        check_vma=False,
    )
```

```python
import functools

import jax
import jax.numpy as jnp
from jax import lax
from jax.experimental import pallas as pl
from jax.experimental.pallas import tpu as pltpu
from jax.sharding import PartitionSpec as P

MESH = pl.DeviceIdType.MESH
F32, BF16 = jnp.float32, jnp.bfloat16

NX, NC = 4, 2
KW, HV, SEG = 128, 256, 64
HEADS = 2
ROWS = 256
SEGS = ROWS // SEG
NCHUNK = 8
CW = 256
W, S = 1, 0
X_ORDER = (1, 3, 2)
NEAR = (1, 2, 3)
W_GREETINGS, S_GREETINGS = 12, 14
A_SEND = (3, -2, 2, -1, 1)
B_SEND = (5, -5)
Z_SENDS = {
    0: (1, -1, 4, -4), 1: (-1,), -1: (1,), 4: (1, -1), -4: (1, -1),
    5: (-1,), -5: (1,), 6: (-1,), -6: (1,), 7: (-1,),
}
ARRIVE, RELAY, FINISH, CONV = range(4)
ROW_ORDER = (0, -1, 1, 4, -2, -4, 2, 5, -5, -6, 6, -3, 3, 7, 8, -7)
BEFORE_STATES = (
    (ARRIVE, 1), (ARRIVE, -1), (RELAY, 0), (ARRIVE, 4), (RELAY, 1), (RELAY, -1),
    (CONV, 0), (ARRIVE, -2), (ARRIVE, 2), (ARRIVE, -4), (RELAY, 4), (FINISH, 0),
    (ARRIVE, 5), (ARRIVE, -3), (FINISH, -1), (FINISH, 1), (RELAY, -2), (ARRIVE, -5),
    (RELAY, -4), (RELAY, 2), (ARRIVE, 6), (RELAY, 5), (FINISH, 4), (ARRIVE, -6),
    (ARRIVE, 3), (FINISH, -2), (RELAY, -5), (ARRIVE, 7), (ARRIVE, -7), (FINISH, -4),
    (FINISH, 2), (RELAY, -6), (FINISH, 5), (RELAY, -3), (ARRIVE, 8), (RELAY, 6),
    (RELAY, 3), (FINISH, -5), (RELAY, 7), (RELAY, -7), (RELAY, 8),
)
W_COMBINES = ((), (), (), (), (), (), (), tuple(range(8)))
S_COMBINES = ((), (), (), (0,), (), (1,), (), (2, 3, 4, 5, 6, 7))
LAST_ROWS = ((-6, 6), (-3, 3), (7,), (8, -7), (), (), (), ())
NT = (((1,), (1,)), ((), ()))
TN = (((0,), (0,)), ((), ()))


def terms(a):
    high = a.astype(BF16).astype(F32)
    rest = a - high
    mid = rest.astype(BF16).astype(F32)
    return [high, mid, rest - mid]


def decay_rows(*decays):
    rows = [r for a in decays for r in terms(a)]
    rows.append(jnp.zeros((16 - len(rows), KW), F32))
    return jnp.concatenate(rows, axis=0).astype(BF16)


def decay_of(block, which=0):
    b = block.astype(F32)
    i = 3 * which
    return b[i : i + 1] + b[i + 1 : i + 2] + b[i + 2 : i + 3]


def chain(earlier, latter):
    return earlier[0] * latter[0], latter[0] * earlier[1] + latter[1]


def only_if(valid, pair):
    return jnp.where(valid, pair[0], 1.0), jnp.where(valid, pair[1], 0.0)


def layer_kernel(
    nz,
    nt,
    q_in, k_in, v_in, code_in, up_in, bias_in, gain_in, cin_in, cgate_in, taps_in,
    wgla_in, wconv_in,
    out,
    q, k, v, code, up, bias, gain, cin, cgate, taps,
    wt, states, through, ubuf, u0, pbuf, prec, abuf, arec, wbuf, brec, rbuf, sin,
    ctail, ext, mix, wblk, sout, part, rel, comb, from_left, from_right,
    zsem, fsem, ws_sem, fs_sem, wd_sem,
    u0_sem, p_sem, a_sem, b_sem, r_sem, sin_sem, c_sem,
    rel_sem, left_sem, right_sem, tail_send, load_sem, wload_sem,
):
    s = lax.axis_index("sp")
    t = lax.axis_index("tp")
    ns = nz * NX * NC
    c = lax.rem(s, NC)
    x = lax.rem(s // NC, NX)
    z = s // (NC * NX)

    def chip(zz, xx, cc):
        return {"sp": (zz * NX + xx) * NC + cc, "tp": t}

    def along_z(d):
        return chip(lax.rem(z + d + nz, nz), x, c)

    def along_x(d):
        return chip(z, lax.rem(x + d + NX, NX), c)

    def along_y(d):
        return {"sp": s, "tp": lax.rem(t + d + nt, nt)}

    def next_in_order(d):
        return {"sp": lax.rem(s + d + ns, ns), "tp": t}

    partner = chip(z, x, 1 - c)

    def rdma(src, dst, send, recv, dev):
        return pltpu.make_async_remote_copy(
            src_ref=src, dst_ref=dst, send_sem=send, recv_sem=recv,
            device_id=dev, device_id_type=MESH,
        )

    barrier = pltpu.get_barrier_semaphore()

    def greet(dev):
        pl.semaphore_signal(barrier, inc=1, device_id=dev, device_id_type=MESH)

    greet(partner)
    for d in (1, 2, 3):
        greet(along_x(d))
    for d in (1, -1):
        greet(along_y(d))
        greet(next_in_order(d))

    @pl.when(c == W)
    def _():
        for d in (1, 4):
            greet(along_z(d))
            greet(along_z(-d))

    @pl.when(c == S)
    def _():
        for d in NEAR:
            greet(along_z(d))
            greet(along_z(-d))

    loads = {
        name: pltpu.make_async_copy(src, dst, load_sem.at[i])
        for i, (name, src, dst) in enumerate((
            ("code", code_in, code), ("up", up_in, up), ("bias", bias_in, bias),
            ("k", k_in, k), ("v", v_in, v), ("cin", cin_in, cin),
            ("cgate", cgate_in, cgate), ("taps", taps_in, taps), ("q", q_in, q),
            ("gain", gain_in, gain),
        ))
    }
    own_rows, other_rows = slice(16 * W, 16 * W + 16), slice(16 * S, 16 * S + 16)
    width = HEADS * HV

    def weight_loads(block):
        return (
            pltpu.make_async_copy(wgla_in, block.at[:, 0:width], wload_sem.at[0]),
            pltpu.make_async_copy(wconv_in, block.at[:, width:], wload_sem.at[1]),
        )

    @pl.when(c == W)
    def _():
        for copy in weight_loads(wt.at[z, x, own_rows]):
            copy.start()

    @pl.when(c == S)
    def _():
        for copy in weight_loads(wblk):
            copy.start()

    for copy in loads.values():
        copy.start()
    for name in ("code", "up", "bias"):
        loads[name].wait()
    score = lax.dot_general(code[...], up[...], TN, preferred_element_type=F32) + bias[...]
    log_decay = (jnp.minimum(score, 0.0) - jnp.log1p(jnp.exp(-jnp.abs(score)))) / 16.0
    row = lax.broadcasted_iota(jnp.int32, (SEG, SEG), 0)
    col = lax.broadcasted_iota(jnp.int32, (SEG, SEG), 1)
    later = (col > row).astype(F32)
    to_end, seg_decays = [], []
    for n in range(SEGS):
        here = log_decay[n * SEG : (n + 1) * SEG]
        rest = jnp.dot(
            later, here, preferred_element_type=F32, precision=lax.Precision.HIGHEST
        )
        to_end.append(jnp.exp(rest))
        seg_decays.append(jnp.exp(rest[0:1] + here[0:1]))

    @pl.when(c == S)
    def _():
        for copy in weight_loads(wblk):
            copy.wait()
        pl.semaphore_wait(barrier, S_GREETINGS)
        rdma(wblk, wt.at[z, x, other_rows], wd_sem.at[0], wd_sem.at[1], partner).start()

    loads["k"].wait()
    loads["v"].wait()
    acc = [None] * HEADS
    thr = None
    for n in range(SEGS):
        seg_decay = seg_decays[n]
        scaled = (k[n * SEG : (n + 1) * SEG, :].astype(F32) * to_end[n]).astype(BF16)
        thr = seg_decay if n == 0 else thr * seg_decay
        through[n] = jnp.broadcast_to(thr, (8, HEADS * KW))
        for h in range(HEADS):
            update = lax.dot_general(
                v[n * SEG : (n + 1) * SEG, h * HV : (h + 1) * HV],
                scaled[:, h * KW : (h + 1) * KW],
                TN,
                preferred_element_type=F32,
            )
            if n == 0:
                acc[h] = update
            else:
                acc[h] = acc[h] * seg_decay[:, h * KW : (h + 1) * KW] + update
            states[n, h * HV : (h + 1) * HV, :] = acc[h]
    for h in range(HEADS):
        ubuf[h * HV : (h + 1) * HV, :] = acc[h].astype(BF16)
    ubuf[HEADS * HV :, :] = decay_rows(thr[:, :KW], thr[:, KW:])

    @pl.when(c == W)
    def _():
        for copy in weight_loads(wt.at[z, x, own_rows]):
            copy.wait()
        pl.semaphore_wait(barrier, W_GREETINGS)

    tail_copy = rdma(
        cin.at[ROWS - 16 : ROWS], ctail, c_sem.at[0], c_sem.at[1], next_in_order(1)
    )

    def conv():
        loads["cgate"].wait()
        loads["taps"].wait()
        tail_copy.wait_recv()
        ext[8:, :] = cin[...].astype(F32)
        ext[0:8, :] = jnp.where(s == 0, 0.0, ctail[...].astype(F32)[8:16])
        done = taps[0:1] * ext[6 : 6 + ROWS, :]
        done = done + taps[1:2] * ext[7 : 7 + ROWS, :]
        done = done + taps[2:3] * ext[8 : 8 + ROWS, :]
        mix[:, HEADS * HV :] = (cgate[...].astype(F32) * done).astype(BF16)

    def read_out(incoming):
        loads["q"].wait()
        loads["gain"].wait()
        for h in range(HEADS):
            for n in range(SEGS):
                decay = through[n, 0:1, h * KW : (h + 1) * KW]
                state = states[n, h * HV : (h + 1) * HV, :] + decay * incoming(h)
                got = lax.dot_general(
                    q[n * SEG : (n + 1) * SEG, h * KW : (h + 1) * KW],
                    state.astype(BF16),
                    NT,
                    preferred_element_type=F32,
                )
                scale = lax.rsqrt(jnp.mean(got * got, axis=-1, keepdims=True) + 1.0)
                mix[n * SEG : (n + 1) * SEG, h * HV : (h + 1) * HV] = (
                    got * scale * gain[...]
                ).astype(BF16)

    def arrived(h):
        return jnp.concatenate([sin[2 * h], sin[2 * h + 1]], axis=0).astype(F32)

    right, left = along_y(1), along_y(-1)
    opposite, at_right, at_left = (lax.rem(t + d, nt) for d in (2, 1, 3))

    def row_at(d):
        return lax.rem(z + d + nz, nz)

    def rows_of(o):
        return [row_at(d) for d in ROW_ORDER[2 * o : 2 * o + 2]]

    def project(o):
        w = jnp.concatenate([wt[rr].reshape(CW // 2, 2 * width) for rr in rows_of(o)], axis=0)
        got = lax.dot_general(mix[...], w, NT, preferred_element_type=F32)
        part[o] = got.astype(BF16).reshape(nt, ROWS // nt, CW)
        rdma(
            part.at[o, opposite], rel.at[o], tail_send.at[0], rel_sem.at[o],
            right if o % 2 == 0 else left,
        ).start()

    def send_direct(o):
        if o % 2 == 0:
            rdma(
                part.at[o, at_left], from_right.at[o], tail_send.at[1],
                right_sem.at[o], left,
            ).start()
        else:
            rdma(
                part.at[o, at_right], from_left.at[o], tail_send.at[1],
                left_sem.at[o], right,
            ).start()

    def combine(o):
        to = right if o % 2 == 0 else left
        rdma(part.at[o, 0], rel.at[o], tail_send.at[0], rel_sem.at[o], to).wait_recv()
        mine = part[o, at_right if o % 2 == 0 else at_left]
        comb[o] = (rel[o].astype(F32) + mine.astype(F32)).astype(BF16)
        if o % 2 == 0:
            rdma(comb.at[o], from_left.at[o], tail_send.at[2], left_sem.at[o], right).start()
        else:
            rdma(comb.at[o], from_right.at[o], tail_send.at[2], right_sem.at[o], left).start()

    def conclude(o):
        rdma(comb.at[o], from_left.at[o], tail_send.at[2], left_sem.at[o], right).wait_recv()
        rdma(comb.at[o], from_right.at[o], tail_send.at[2], right_sem.at[o], left).wait_recv()
        total = part[o, t].astype(F32) + from_left[o].astype(F32) + from_right[o].astype(F32)
        for i, rr in enumerate(rows_of(o)):
            half = CW // 2
            out[:, pl.ds(pl.multiple_of(rr * half, half), half)] = total[
                :, i * half : (i + 1) * half
            ].astype(BF16)

    def send_block(rr, xx, sem, dev):
        block = wt.at[rr, xx]
        rdma(block, block, ws_sem.at[sem], zsem.at[rr, xx], dev).start()

    def wait_block(rr, xx):
        block = wt.at[rr, xx]
        rdma(block, block, ws_sem.at[0], zsem.at[rr, xx], partner).wait_recv()

    def x_at(d):
        return lax.rem(x + d, NX)

    def arrive(d):
        if d != 0:
            wait_block(row_at(d), x)
        for to in Z_SENDS.get(d, ()):
            send_block(row_at(d), x, 0, along_z(to))
        for to in (1, 3):
            send_block(row_at(d), x, 1, along_x(to))

    def relay(d):
        near = 3 if d <= 0 else 1
        wait_block(row_at(d), x_at(near))
        send_block(row_at(d), x_at(near), 2, along_x(4 - near))

    def finish(d):
        far = 1 if d <= 0 else 3
        wait_block(row_at(d), x_at(far))
        wait_block(row_at(d), x_at(2))
        rr = row_at(d)
        rdma(wt.at[rr], wt.at[rr], fs_sem, fsem.at[rr], partner).start()

    @pl.when(c == W)
    def _():
        rdma(ubuf, u0, u0_sem.at[0], u0_sem.at[1], partner).start()
        loads["cin"].wait()
        tail_copy.start()
        rdma(wblk, wt.at[z, x, other_rows], wd_sem.at[0], wd_sem.at[1], partner).wait_recv()
        arrive(0)
        for what, d in BEFORE_STATES:
            (arrive, relay, finish, lambda _: conv())[what](d)
        rdma(sin, sin, sin_sem.at[0], sin_sem.at[1], partner).wait_recv()
        read_out(arrived)
        for o in range(NCHUNK):
            project(o)
            for d in LAST_ROWS[o]:
                finish(d)
            send_direct(o)
            for i in W_COMBINES[o]:
                combine(i)

    @pl.when(c == S)
    def _():
        loads["cin"].wait()
        tail_copy.start()
        rdma(ubuf, u0, u0_sem.at[0], u0_sem.at[1], partner).wait_recv()

        def theirs(h, lo, hi):
            return (
                decay_of(u0[HEADS * HV :, :], h),
                u0[h * HV + lo : h * HV + hi, :].astype(F32),
            )

        def ours(h, lo, hi):
            return thr[:, h * KW : (h + 1) * KW], acc[h][lo:hi]

        first, second = (theirs, ours) if S == 1 else (ours, theirs)
        for i in range(NX):
            part_of = (i // 2, (i % 2) * KW, (i % 2 + 1) * KW)
            both = chain(first(*part_of), second(*part_of))
            pbuf[i, 0:KW, :] = both[1].astype(BF16)
            pbuf[i, KW:, :] = decay_rows(both[0])
        for d in (2, 1, 3):
            rdma(
                pbuf.at[lax.rem(x + d, NX)], prec.at[x],
                p_sem.at[0], p_sem.at[1 + d], along_x(d),
            ).start()
        prec[x] = pbuf[x]
        for d in (1, 2, 3):
            rdma(
                pbuf.at[0], prec.at[lax.rem(x - d + NX, NX)],
                p_sem.at[0], p_sem.at[1 + d], along_x(d),
            ).wait_recv()

        def pair_in(ref, i):
            return decay_of(ref[i, KW:, :]), ref[i, 0:KW, :].astype(F32)

        chips = [pair_in(prec, i) for i in range(NX)]
        plane = chips[0]
        for i in range(1, NX):
            plane = chain(plane, chips[i])
        abuf[0:KW, :] = plane[1].astype(BF16)
        abuf[KW:, :] = decay_rows(plane[0])
        for j, d in enumerate(A_SEND):
            rdma(abuf, arec.at[j], a_sem.at[5], a_sem.at[j], along_z(d)).start()
        conv()
        for j, d in enumerate(A_SEND):
            rdma(abuf, arec.at[j], a_sem.at[5], a_sem.at[j], along_z(d)).wait_recv()
        back3, ahead2, back2, ahead1, back1 = (pair_in(arec, j) for j in range(5))
        inner = z <= nz - 6
        window = chain(
            only_if(inner & (z >= 2), back2), only_if(inner & (z >= 1), back1)
        )
        window = chain(window, only_if(inner, plane))
        window = chain(window, only_if(inner | (z == nz - 1), ahead1))
        window = chain(window, only_if(inner | (z >= nz - 2), ahead2))
        wider = chain(only_if(inner & (z >= 3), back3), window)
        for j, (decay, state) in enumerate((wider, window)):
            wbuf[j, 0:KW, :] = state.astype(BF16)
            wbuf[j, KW:, :] = decay_rows(decay)
        for j, d in enumerate(B_SEND):
            rdma(wbuf.at[j], brec.at[j], b_sem.at[2], b_sem.at[j], along_z(d)).start()
        oldest = chain(only_if(z >= nz - 1, ahead1), only_if(z >= nz - 2, ahead2))
        newest = chain(only_if(z >= 2, back2), only_if(z >= 1, back1))
        for j, d in enumerate(B_SEND):
            rdma(wbuf.at[j], brec.at[j], b_sem.at[2], b_sem.at[j], along_z(d)).wait_recv()
        before = chain(oldest, only_if(z >= 9, pair_in(brec, 1)))
        before = chain(before, only_if(z >= 3, pair_in(brec, 0)))
        before = chain(before, newest)
        run = before[1]
        for i in range(NX):
            rbuf[i] = run.astype(BF16)
            if i < NX - 1:
                run = chips[i][0] * run + chips[i][1]
        for d in (2, 1, 3):
            rdma(
                rbuf.at[lax.rem(x + d, NX)], sin.at[x],
                r_sem.at[0], r_sem.at[1 + d], along_x(d),
            ).start()
        sin[x] = rbuf[x]
        for d in (1, 2, 3):
            rdma(
                rbuf.at[0], sin.at[lax.rem(x - d + NX, NX)],
                r_sem.at[0], r_sem.at[1 + d], along_x(d),
            ).wait_recv()

        def after_first(h):
            decay, update = first(h, 0, HV)
            return decay * arrived(h) + update

        if S == 1:
            rdma(sin, sin, sin_sem.at[0], sin_sem.at[1], partner).start()
        else:
            for h in range(HEADS):
                sout[2 * h : 2 * h + 2] = after_first(h).astype(BF16).reshape(2, KW, KW)
            rdma(sout, sin, sin_sem.at[0], sin_sem.at[1], partner).start()
        read_out(after_first if S == 1 else arrived)
        for o in range(NCHUNK):
            for rr in rows_of(o):
                rdma(wt.at[rr], wt.at[rr], fs_sem, fsem.at[rr], partner).wait_recv()
            project(o)
            send_direct(o)
            for i in S_COMBINES[o]:
                combine(i)

    for o in range(NCHUNK):
        conclude(o)
    for i in range(3):
        rdma(comb, rel, tail_send.at[i], rel_sem.at[0], right).wait_send()
    tail_copy.wait_send()

    @pl.when(c == W)
    def _():
        rdma(ubuf, u0, u0_sem.at[0], u0_sem.at[1], partner).wait_send()
        for sem, ref in enumerate((wt.at[0:15, 0], wt.at[0:8], wt.at[0:4])):
            rdma(ref, ref, ws_sem.at[sem], zsem.at[0, 0], partner).wait_send()
        rdma(wt, wt, fs_sem, fsem.at[0], partner).wait_send()

    @pl.when(c == S)
    def _():
        rdma(wblk, wt.at[0, 0, 0:16], wd_sem.at[0], wd_sem.at[1], partner).wait_send()
        rdma(pbuf.at[0:3], prec.at[0:3], p_sem.at[0], p_sem.at[1], partner).wait_send()
        rdma(arec, arec, a_sem.at[5], a_sem.at[0], partner).wait_send()
        rdma(brec, brec, b_sem.at[2], b_sem.at[0], partner).wait_send()
        rdma(rbuf.at[0:3], sin.at[0:3], r_sem.at[0], r_sem.at[1], partner).wait_send()
        rdma(sin, sin, sin_sem.at[0], sin_sem.at[1], partner).wait_send()


def solution(mesh):
    nt = mesh.shape["tp"]
    nz = mesh.shape["sp"] // (NX * NC)

    def step(
        queries, keys, values, gate_code, gate_up, gate_bias, gla_gain,
        conv_input, conv_gate, conv_taps, out_gla, out_conv,
    ):
        width = HEADS * HV
        vm, dma = pltpu.VMEM, pltpu.SemaphoreType.DMA
        quarter = ROWS // nt
        scratch = [
            vm((ROWS, HEADS * KW), BF16),
            vm((ROWS, HEADS * KW), BF16),
            vm((ROWS, width), BF16),
            vm((32, ROWS), BF16),
            vm((32, HEADS * KW), BF16),
            vm((1, HEADS * KW), F32),
            vm((1, HV), F32),
            vm((ROWS, width), BF16),
            vm((ROWS, width), BF16),
            vm((3, width), F32),
            vm((nz, NX, 32, 2 * width), BF16),
            vm((SEGS, width, KW), F32),
            vm((SEGS, 8, HEADS * KW), F32),
            vm((width + 16, KW), BF16),
            vm((width + 16, KW), BF16),
            vm((NX, KW + 16, KW), BF16),
            vm((NX, KW + 16, KW), BF16),
            vm((KW + 16, KW), BF16),
            vm((5, KW + 16, KW), BF16),
            vm((2, KW + 16, KW), BF16),
            vm((2, KW + 16, KW), BF16),
            vm((NX, KW, KW), BF16),
            vm((NX, KW, KW), BF16),
            vm((16, width), BF16),
            vm((8 + ROWS, width), F32),
            vm((ROWS, 2 * width), BF16),
            vm((16, 2 * width), BF16),
            vm((NX, KW, KW), BF16),
            vm((NCHUNK, nt, quarter, CW), BF16),
            vm((NCHUNK, quarter, CW), BF16),
            vm((NCHUNK, quarter, CW), BF16),
            vm((NCHUNK, quarter, CW), BF16),
            vm((NCHUNK, quarter, CW), BF16),
            dma((nz, NX)), dma((nz,)), dma((3,)), dma, dma((2,)),
            dma((2,)), dma((5,)), dma((6,)), dma((3,)), dma((5,)), dma((2,)), dma((2,)),
            dma((NCHUNK,)), dma((NCHUNK,)), dma((NCHUNK,)), dma((3,)), dma((10,)), dma((2,)),
        ]
        return pl.pallas_call(
            functools.partial(layer_kernel, nz, nt),
            out_shape=pltpu.VMEM((quarter, 2048), BF16),
            in_specs=[pl.BlockSpec(memory_space=pl.ANY)] * 12,
            out_specs=pl.BlockSpec(memory_space=pltpu.VMEM),
            scratch_shapes=scratch,
            compiler_params=pltpu.CompilerParams(collective_id=0, has_side_effects=True),
            name="layer",
        )(
            queries, keys, values, gate_code.T, gate_up, gate_bias[None], gla_gain[None],
            conv_input, conv_gate, conv_taps, out_gla.T, out_conv.T,
        )

    return jax.shard_map(
        step,
        mesh=mesh,
        in_specs=(
            P("sp", "tp"), P("sp", "tp"), P("sp", "tp"), P("sp", None), P(None, "tp"),
            P("tp"), P(), P("sp", "tp"), P("sp", "tp"), P(None, "tp"),
            P("tp", "sp"), P("tp", "sp"),
        ),
        out_specs=P(("sp", "tp"), None),
        check_vma=False,
    )
```

```python
import functools

import jax
import jax.numpy as jnp
from jax import lax
from jax.experimental import pallas as pl
from jax.experimental.pallas import tpu as pltpu
from jax.sharding import PartitionSpec as P

MESH = pl.DeviceIdType.MESH
F32, BF16 = jnp.float32, jnp.bfloat16

NX, NC = 4, 2
KW, HV, SEG = 128, 256, 64
HEADS = 2
ROWS = 256
SEGS = ROWS // SEG
NCHUNK = 8
CW = 256
W, S = 1, 0
X_ORDER = (1, 3, 2)
NEAR = (1, 2, 3)
W_GREETINGS, S_GREETINGS = 12, 14
A_SEND = (3, -2, 2, -1, 1)
B_SEND = (5, -5)
Z_SENDS = {
    0: (1, -1, 4, -4), 1: (-1,), -1: (1,), 4: (1, -1), -4: (1, -1),
    5: (-1,), -5: (1,), 6: (-1,), -6: (1,), 7: (-1,),
}
ARRIVE, RELAY, FINISH, CONV = range(4)
ROW_ORDER = (0, -1, 1, 4, -2, -4, 2, 5, -5, -6, 6, -3, 3, 7, 8, -7)
BEFORE_STATES = (
    (ARRIVE, 1), (ARRIVE, -1), (RELAY, 0), (ARRIVE, 4), (RELAY, 1), (RELAY, -1),
    (CONV, 0), (ARRIVE, -2), (ARRIVE, 2), (ARRIVE, -4), (RELAY, 4), (FINISH, 0),
    (ARRIVE, 5), (ARRIVE, -3), (FINISH, -1), (FINISH, 1), (RELAY, -2), (ARRIVE, -5),
    (RELAY, -4), (RELAY, 2), (ARRIVE, 6), (RELAY, 5), (FINISH, 4), (ARRIVE, -6),
    (ARRIVE, 3), (FINISH, -2), (RELAY, -5), (ARRIVE, 7), (ARRIVE, -7), (FINISH, -4),
    (FINISH, 2), (RELAY, -6), (FINISH, 5), (RELAY, -3), (ARRIVE, 8), (RELAY, 6),
    (RELAY, 3), (FINISH, -5), (RELAY, 7), (RELAY, -7), (RELAY, 8), (FINISH, -6), (FINISH, 6),
)
W_COMBINES = ((), (), (), (), (), (), (), tuple(range(8)))
S_COMBINES = ((), (), (), (0,), (), (1,), (), (2, 3, 4, 5, 6, 7))
LAST_ROWS = ((-3,), (3, 7), (8,), (-7,), (), (), (), ())
NT = (((1,), (1,)), ((), ()))
TN = (((0,), (0,)), ((), ()))


def terms(a):
    high = a.astype(BF16).astype(F32)
    rest = a - high
    mid = rest.astype(BF16).astype(F32)
    return [high, mid, rest - mid]


def decay_rows(*decays):
    rows = [r for a in decays for r in terms(a)]
    rows.append(jnp.zeros((16 - len(rows), KW), F32))
    return jnp.concatenate(rows, axis=0).astype(BF16)


def decay_of(block, which=0):
    b = block.astype(F32)
    i = 3 * which
    return b[i : i + 1] + b[i + 1 : i + 2] + b[i + 2 : i + 3]


def chain(earlier, latter):
    return earlier[0] * latter[0], latter[0] * earlier[1] + latter[1]


def only_if(valid, pair):
    return jnp.where(valid, pair[0], 1.0), jnp.where(valid, pair[1], 0.0)


def layer_kernel(
    nz,
    nt,
    q_in, k_in, v_in, code_in, up_in, bias_in, gain_in, cin_in, cgate_in, taps_in,
    wgla_in, wconv_in,
    out,
    q, k, v, code, up, bias, gain, cin, cgate, taps,
    wt, states, through, ubuf, u0, pbuf, prec, abuf, arec, wbuf, brec, rbuf, sin,
    ctail, ext, mix, wblk, sout, part, rel, comb, from_left, from_right,
    zsem, fsem, ws_sem, fs_sem, wd_sem,
    u0_sem, p_sem, a_sem, b_sem, r_sem, sin_sem, c_sem,
    rel_sem, left_sem, right_sem, tail_send, load_sem, wload_sem,
):
    s = lax.axis_index("sp")
    t = lax.axis_index("tp")
    ns = nz * NX * NC
    c = lax.rem(s, NC)
    x = lax.rem(s // NC, NX)
    z = s // (NC * NX)

    def chip(zz, xx, cc):
        return {"sp": (zz * NX + xx) * NC + cc, "tp": t}

    def along_z(d):
        return chip(lax.rem(z + d + nz, nz), x, c)

    def along_x(d):
        return chip(z, lax.rem(x + d + NX, NX), c)

    def along_y(d):
        return {"sp": s, "tp": lax.rem(t + d + nt, nt)}

    def next_in_order(d):
        return {"sp": lax.rem(s + d + ns, ns), "tp": t}

    partner = chip(z, x, 1 - c)

    def rdma(src, dst, send, recv, dev):
        return pltpu.make_async_remote_copy(
            src_ref=src, dst_ref=dst, send_sem=send, recv_sem=recv,
            device_id=dev, device_id_type=MESH,
        )

    barrier = pltpu.get_barrier_semaphore()

    def greet(dev):
        pl.semaphore_signal(barrier, inc=1, device_id=dev, device_id_type=MESH)

    greet(partner)
    for d in (1, 2, 3):
        greet(along_x(d))
    for d in (1, -1):
        greet(along_y(d))
        greet(next_in_order(d))

    @pl.when(c == W)
    def _():
        for d in (1, 4):
            greet(along_z(d))
            greet(along_z(-d))

    @pl.when(c == S)
    def _():
        for d in NEAR:
            greet(along_z(d))
            greet(along_z(-d))

    loads = {
        name: pltpu.make_async_copy(src, dst, load_sem.at[i])
        for i, (name, src, dst) in enumerate((
            ("code", code_in, code), ("up", up_in, up), ("bias", bias_in, bias),
            ("k", k_in, k), ("v", v_in, v), ("cin", cin_in, cin),
            ("cgate", cgate_in, cgate), ("taps", taps_in, taps), ("q", q_in, q),
            ("gain", gain_in, gain),
        ))
    }
    own_rows, other_rows = slice(16 * W, 16 * W + 16), slice(16 * S, 16 * S + 16)
    width = HEADS * HV

    def weight_loads(block):
        return (
            pltpu.make_async_copy(wgla_in, block.at[:, 0:width], wload_sem.at[0]),
            pltpu.make_async_copy(wconv_in, block.at[:, width:], wload_sem.at[1]),
        )

    @pl.when(c == W)
    def _():
        for copy in weight_loads(wt.at[z, x, own_rows]):
            copy.start()

    @pl.when(c == S)
    def _():
        for copy in weight_loads(wblk):
            copy.start()

    for copy in loads.values():
        copy.start()
    for name in ("code", "up", "bias"):
        loads[name].wait()
    score = lax.dot_general(code[...], up[...], TN, preferred_element_type=F32) + bias[...]
    log_decay = (jnp.minimum(score, 0.0) - jnp.log1p(jnp.exp(-jnp.abs(score)))) / 16.0
    row = lax.broadcasted_iota(jnp.int32, (SEG, SEG), 0)
    col = lax.broadcasted_iota(jnp.int32, (SEG, SEG), 1)
    later = (col > row).astype(F32)
    to_end, seg_decays = [], []
    for n in range(SEGS):
        here = log_decay[n * SEG : (n + 1) * SEG]
        rest = jnp.dot(
            later, here, preferred_element_type=F32, precision=lax.Precision.HIGHEST
        )
        to_end.append(jnp.exp(rest))
        seg_decays.append(jnp.exp(rest[0:1] + here[0:1]))

    @pl.when(c == S)
    def _():
        for copy in weight_loads(wblk):
            copy.wait()
        pl.semaphore_wait(barrier, S_GREETINGS)
        rdma(wblk, wt.at[z, x, other_rows], wd_sem.at[0], wd_sem.at[1], partner).start()

    loads["k"].wait()
    loads["v"].wait()
    acc = [None] * HEADS
    thr = None
    for n in range(SEGS):
        seg_decay = seg_decays[n]
        scaled = (k[n * SEG : (n + 1) * SEG, :].astype(F32) * to_end[n]).astype(BF16)
        thr = seg_decay if n == 0 else thr * seg_decay
        through[n] = jnp.broadcast_to(thr, (8, HEADS * KW))
        for h in range(HEADS):
            update = lax.dot_general(
                v[n * SEG : (n + 1) * SEG, h * HV : (h + 1) * HV],
                scaled[:, h * KW : (h + 1) * KW],
                TN,
                preferred_element_type=F32,
            )
            if n == 0:
                acc[h] = update
            else:
                acc[h] = acc[h] * seg_decay[:, h * KW : (h + 1) * KW] + update
            states[n, h * HV : (h + 1) * HV, :] = acc[h]
    for h in range(HEADS):
        ubuf[h * HV : (h + 1) * HV, :] = acc[h].astype(BF16)
    ubuf[HEADS * HV :, :] = decay_rows(thr[:, :KW], thr[:, KW:])

    @pl.when(c == W)
    def _():
        for copy in weight_loads(wt.at[z, x, own_rows]):
            copy.wait()
        pl.semaphore_wait(barrier, W_GREETINGS)

    tail_copy = rdma(
        cin.at[ROWS - 16 : ROWS], ctail, c_sem.at[0], c_sem.at[1], next_in_order(1)
    )

    def conv():
        loads["cgate"].wait()
        loads["taps"].wait()
        tail_copy.wait_recv()
        ext[8:, :] = cin[...].astype(F32)
        ext[0:8, :] = jnp.where(s == 0, 0.0, ctail[...].astype(F32)[8:16])
        done = taps[0:1] * ext[6 : 6 + ROWS, :]
        done = done + taps[1:2] * ext[7 : 7 + ROWS, :]
        done = done + taps[2:3] * ext[8 : 8 + ROWS, :]
        mix[:, HEADS * HV :] = (cgate[...].astype(F32) * done).astype(BF16)

    def read_out(incoming):
        loads["q"].wait()
        loads["gain"].wait()
        for h in range(HEADS):
            for n in range(SEGS):
                decay = through[n, 0:1, h * KW : (h + 1) * KW]
                state = states[n, h * HV : (h + 1) * HV, :] + decay * incoming(h)
                got = lax.dot_general(
                    q[n * SEG : (n + 1) * SEG, h * KW : (h + 1) * KW],
                    state.astype(BF16),
                    NT,
                    preferred_element_type=F32,
                )
                scale = lax.rsqrt(jnp.mean(got * got, axis=-1, keepdims=True) + 1.0)
                mix[n * SEG : (n + 1) * SEG, h * HV : (h + 1) * HV] = (
                    got * scale * gain[...]
                ).astype(BF16)

    def arrived(h):
        return jnp.concatenate([sin[2 * h], sin[2 * h + 1]], axis=0).astype(F32)

    right, left = along_y(1), along_y(-1)
    opposite, at_right, at_left = (lax.rem(t + d, nt) for d in (2, 1, 3))

    def row_at(d):
        return lax.rem(z + d + nz, nz)

    def rows_of(o):
        return [row_at(d) for d in ROW_ORDER[2 * o : 2 * o + 2]]

    def project(o):
        w = jnp.concatenate([wt[rr].reshape(CW // 2, 2 * width) for rr in rows_of(o)], axis=0)
        got = lax.dot_general(mix[...], w, NT, preferred_element_type=F32)
        part[o] = got.astype(BF16).reshape(nt, ROWS // nt, CW)
        rdma(
            part.at[o, opposite], rel.at[o], tail_send.at[0], rel_sem.at[o],
            right if o % 2 == 0 else left,
        ).start()

    def send_direct(o):
        if o % 2 == 0:
            rdma(
                part.at[o, at_left], from_right.at[o], tail_send.at[1],
                right_sem.at[o], left,
            ).start()
        else:
            rdma(
                part.at[o, at_right], from_left.at[o], tail_send.at[1],
                left_sem.at[o], right,
            ).start()

    def combine(o):
        to = right if o % 2 == 0 else left
        rdma(part.at[o, 0], rel.at[o], tail_send.at[0], rel_sem.at[o], to).wait_recv()
        mine = part[o, at_right if o % 2 == 0 else at_left]
        comb[o] = (rel[o].astype(F32) + mine.astype(F32)).astype(BF16)
        if o % 2 == 0:
            rdma(comb.at[o], from_left.at[o], tail_send.at[2], left_sem.at[o], right).start()
        else:
            rdma(comb.at[o], from_right.at[o], tail_send.at[2], right_sem.at[o], left).start()

    def conclude(o):
        rdma(comb.at[o], from_left.at[o], tail_send.at[2], left_sem.at[o], right).wait_recv()
        rdma(comb.at[o], from_right.at[o], tail_send.at[2], right_sem.at[o], left).wait_recv()
        total = part[o, t].astype(F32) + from_left[o].astype(F32) + from_right[o].astype(F32)
        for i, rr in enumerate(rows_of(o)):
            half = CW // 2
            out[:, pl.ds(pl.multiple_of(rr * half, half), half)] = total[
                :, i * half : (i + 1) * half
            ].astype(BF16)

    def send_block(rr, xx, sem, dev):
        block = wt.at[rr, xx]
        rdma(block, block, ws_sem.at[sem], zsem.at[rr, xx], dev).start()

    def wait_block(rr, xx):
        block = wt.at[rr, xx]
        rdma(block, block, ws_sem.at[0], zsem.at[rr, xx], partner).wait_recv()

    def x_at(d):
        return lax.rem(x + d, NX)

    def arrive(d):
        if d != 0:
            wait_block(row_at(d), x)
        for to in Z_SENDS.get(d, ()):
            send_block(row_at(d), x, 0, along_z(to))
        for to in (1, 3):
            send_block(row_at(d), x, 1, along_x(to))

    def relay(d):
        near = 3 if d <= 0 else 1
        wait_block(row_at(d), x_at(near))
        send_block(row_at(d), x_at(near), 2, along_x(4 - near))

    def finish(d):
        far = 1 if d <= 0 else 3
        wait_block(row_at(d), x_at(far))
        wait_block(row_at(d), x_at(2))
        rr = row_at(d)
        rdma(wt.at[rr], wt.at[rr], fs_sem, fsem.at[rr], partner).start()

    @pl.when(c == W)
    def _():
        rdma(ubuf, u0, u0_sem.at[0], u0_sem.at[1], partner).start()
        loads["cin"].wait()
        tail_copy.start()
        rdma(wblk, wt.at[z, x, other_rows], wd_sem.at[0], wd_sem.at[1], partner).wait_recv()
        arrive(0)
        for what, d in BEFORE_STATES:
            (arrive, relay, finish, lambda _: conv())[what](d)
        rdma(sin, sin, sin_sem.at[0], sin_sem.at[1], partner).wait_recv()
        read_out(arrived)
        for o in range(NCHUNK):
            project(o)
            for d in LAST_ROWS[o]:
                finish(d)
            send_direct(o)
            for i in W_COMBINES[o]:
                combine(i)

    @pl.when(c == S)
    def _():
        loads["cin"].wait()
        tail_copy.start()
        rdma(ubuf, u0, u0_sem.at[0], u0_sem.at[1], partner).wait_recv()

        def theirs(h, lo, hi):
            return (
                decay_of(u0[HEADS * HV :, :], h),
                u0[h * HV + lo : h * HV + hi, :].astype(F32),
            )

        def ours(h, lo, hi):
            return thr[:, h * KW : (h + 1) * KW], acc[h][lo:hi]

        first, second = (theirs, ours) if S == 1 else (ours, theirs)
        for i in range(NX):
            part_of = (i // 2, (i % 2) * KW, (i % 2 + 1) * KW)
            both = chain(first(*part_of), second(*part_of))
            pbuf[i, 0:KW, :] = both[1].astype(BF16)
            pbuf[i, KW:, :] = decay_rows(both[0])
        for d in (2, 1, 3):
            rdma(
                pbuf.at[lax.rem(x + d, NX)], prec.at[x],
                p_sem.at[0], p_sem.at[1 + d], along_x(d),
            ).start()
        prec[x] = pbuf[x]
        for d in (1, 2, 3):
            rdma(
                pbuf.at[0], prec.at[lax.rem(x - d + NX, NX)],
                p_sem.at[0], p_sem.at[1 + d], along_x(d),
            ).wait_recv()

        def pair_in(ref, i):
            return decay_of(ref[i, KW:, :]), ref[i, 0:KW, :].astype(F32)

        chips = [pair_in(prec, i) for i in range(NX)]
        plane = chips[0]
        for i in range(1, NX):
            plane = chain(plane, chips[i])
        abuf[0:KW, :] = plane[1].astype(BF16)
        abuf[KW:, :] = decay_rows(plane[0])
        for j, d in enumerate(A_SEND):
            rdma(abuf, arec.at[j], a_sem.at[5], a_sem.at[j], along_z(d)).start()
        conv()
        for j, d in enumerate(A_SEND):
            rdma(abuf, arec.at[j], a_sem.at[5], a_sem.at[j], along_z(d)).wait_recv()
        back3, ahead2, back2, ahead1, back1 = (pair_in(arec, j) for j in range(5))
        inner = z <= nz - 6
        window = chain(
            only_if(inner & (z >= 2), back2), only_if(inner & (z >= 1), back1)
        )
        window = chain(window, only_if(inner, plane))
        window = chain(window, only_if(inner | (z == nz - 1), ahead1))
        window = chain(window, only_if(inner | (z >= nz - 2), ahead2))
        wider = chain(only_if(inner & (z >= 3), back3), window)
        for j, (decay, state) in enumerate((wider, window)):
            wbuf[j, 0:KW, :] = state.astype(BF16)
            wbuf[j, KW:, :] = decay_rows(decay)
        for j, d in enumerate(B_SEND):
            rdma(wbuf.at[j], brec.at[j], b_sem.at[2], b_sem.at[j], along_z(d)).start()
        oldest = chain(only_if(z >= nz - 1, ahead1), only_if(z >= nz - 2, ahead2))
        newest = chain(only_if(z >= 2, back2), only_if(z >= 1, back1))
        for j, d in enumerate(B_SEND):
            rdma(wbuf.at[j], brec.at[j], b_sem.at[2], b_sem.at[j], along_z(d)).wait_recv()
        before = chain(oldest, only_if(z >= 9, pair_in(brec, 1)))
        before = chain(before, only_if(z >= 3, pair_in(brec, 0)))
        before = chain(before, newest)
        run = before[1]
        for i in range(NX):
            rbuf[i] = run.astype(BF16)
            if i < NX - 1:
                run = chips[i][0] * run + chips[i][1]
        for d in (2, 1, 3):
            rdma(
                rbuf.at[lax.rem(x + d, NX)], sin.at[x],
                r_sem.at[0], r_sem.at[1 + d], along_x(d),
            ).start()
        sin[x] = rbuf[x]
        for d in (1, 2, 3):
            rdma(
                rbuf.at[0], sin.at[lax.rem(x - d + NX, NX)],
                r_sem.at[0], r_sem.at[1 + d], along_x(d),
            ).wait_recv()

        def after_first(h):
            decay, update = first(h, 0, HV)
            return decay * arrived(h) + update

        if S == 1:
            rdma(sin, sin, sin_sem.at[0], sin_sem.at[1], partner).start()
        else:
            for h in range(HEADS):
                sout[2 * h : 2 * h + 2] = after_first(h).astype(BF16).reshape(2, KW, KW)
            rdma(sout, sin, sin_sem.at[0], sin_sem.at[1], partner).start()
        read_out(after_first if S == 1 else arrived)
        for o in range(NCHUNK):
            for rr in rows_of(o):
                rdma(wt.at[rr], wt.at[rr], fs_sem, fsem.at[rr], partner).wait_recv()
            project(o)
            send_direct(o)
            for i in S_COMBINES[o]:
                combine(i)

    for o in range(NCHUNK):
        conclude(o)
    for i in range(3):
        rdma(comb, rel, tail_send.at[i], rel_sem.at[0], right).wait_send()
    tail_copy.wait_send()

    @pl.when(c == W)
    def _():
        rdma(ubuf, u0, u0_sem.at[0], u0_sem.at[1], partner).wait_send()
        for sem, ref in enumerate((wt.at[0:15, 0], wt.at[0:8], wt.at[0:4])):
            rdma(ref, ref, ws_sem.at[sem], zsem.at[0, 0], partner).wait_send()
        rdma(wt, wt, fs_sem, fsem.at[0], partner).wait_send()

    @pl.when(c == S)
    def _():
        rdma(wblk, wt.at[0, 0, 0:16], wd_sem.at[0], wd_sem.at[1], partner).wait_send()
        rdma(pbuf.at[0:3], prec.at[0:3], p_sem.at[0], p_sem.at[1], partner).wait_send()
        rdma(arec, arec, a_sem.at[5], a_sem.at[0], partner).wait_send()
        rdma(brec, brec, b_sem.at[2], b_sem.at[0], partner).wait_send()
        rdma(rbuf.at[0:3], sin.at[0:3], r_sem.at[0], r_sem.at[1], partner).wait_send()
        rdma(sin, sin, sin_sem.at[0], sin_sem.at[1], partner).wait_send()


def solution(mesh):
    nt = mesh.shape["tp"]
    nz = mesh.shape["sp"] // (NX * NC)

    def step(
        queries, keys, values, gate_code, gate_up, gate_bias, gla_gain,
        conv_input, conv_gate, conv_taps, out_gla, out_conv,
    ):
        width = HEADS * HV
        vm, dma = pltpu.VMEM, pltpu.SemaphoreType.DMA
        quarter = ROWS // nt
        scratch = [
            vm((ROWS, HEADS * KW), BF16),
            vm((ROWS, HEADS * KW), BF16),
            vm((ROWS, width), BF16),
            vm((32, ROWS), BF16),
            vm((32, HEADS * KW), BF16),
            vm((1, HEADS * KW), F32),
            vm((1, HV), F32),
            vm((ROWS, width), BF16),
            vm((ROWS, width), BF16),
            vm((3, width), F32),
            vm((nz, NX, 32, 2 * width), BF16),
            vm((SEGS, width, KW), F32),
            vm((SEGS, 8, HEADS * KW), F32),
            vm((width + 16, KW), BF16),
            vm((width + 16, KW), BF16),
            vm((NX, KW + 16, KW), BF16),
            vm((NX, KW + 16, KW), BF16),
            vm((KW + 16, KW), BF16),
            vm((5, KW + 16, KW), BF16),
            vm((2, KW + 16, KW), BF16),
            vm((2, KW + 16, KW), BF16),
            vm((NX, KW, KW), BF16),
            vm((NX, KW, KW), BF16),
            vm((16, width), BF16),
            vm((8 + ROWS, width), F32),
            vm((ROWS, 2 * width), BF16),
            vm((16, 2 * width), BF16),
            vm((NX, KW, KW), BF16),
            vm((NCHUNK, nt, quarter, CW), BF16),
            vm((NCHUNK, quarter, CW), BF16),
            vm((NCHUNK, quarter, CW), BF16),
            vm((NCHUNK, quarter, CW), BF16),
            vm((NCHUNK, quarter, CW), BF16),
            dma((nz, NX)), dma((nz,)), dma((3,)), dma, dma((2,)),
            dma((2,)), dma((5,)), dma((6,)), dma((3,)), dma((5,)), dma((2,)), dma((2,)),
            dma((NCHUNK,)), dma((NCHUNK,)), dma((NCHUNK,)), dma((3,)), dma((10,)), dma((2,)),
        ]
        return pl.pallas_call(
            functools.partial(layer_kernel, nz, nt),
            out_shape=pltpu.VMEM((quarter, 2048), BF16),
            in_specs=[pl.BlockSpec(memory_space=pl.ANY)] * 12,
            out_specs=pl.BlockSpec(memory_space=pltpu.VMEM),
            scratch_shapes=scratch,
            compiler_params=pltpu.CompilerParams(collective_id=0, has_side_effects=True),
            name="layer",
        )(
            queries, keys, values, gate_code.T, gate_up, gate_bias[None], gla_gain[None],
            conv_input, conv_gate, conv_taps, out_gla.T, out_conv.T,
        )

    return jax.shard_map(
        step,
        mesh=mesh,
        in_specs=(
            P("sp", "tp"), P("sp", "tp"), P("sp", "tp"), P("sp", None), P(None, "tp"),
            P("tp"), P(), P("sp", "tp"), P("sp", "tp"), P(None, "tp"),
            P("tp", "sp"), P("tp", "sp"),
        ),
        out_specs=P(("sp", "tp"), None),
        check_vma=False,
    )
```
